32 devices in a mesh: ep: 16 (over z, x, core), tp: 2 (over y).
Axes of the slice: x: 2, y: 2, z: 4, core: 2. Of those that a mesh axis runs over, the one named last changes fastest.
Arguments:
- mix_input: bfloat16 [8192, 1024], P(('ep', 'tp')), may hold values from -6 to 6
- pool_weight: bfloat16 [8, 128, 128], replicated, may hold values from -0.5 to 0.5
- pool_scale: float32 [1024], replicated, may hold values from 0.1 to 1.9
- out_weight: bfloat16 [1024, 2048], replicated, may hold values from -0.1875 to 0.1875
- moe_input: bfloat16 [2048, 2048], P('ep'), may hold values from -6 to 6
- moe_gain: float32 [2048], replicated, may hold values from 0.1 to 1.9
- group_router: bfloat16 [2048, 4], replicated, may hold values from -0.125 to 0.125
- inner_router: bfloat16 [2048, 16], replicated, may hold values from -0.125 to 0.125
- group_pick: int32 [2048], P('ep'), may hold values from 0 to 3
- inner_pick: int32 [2048, 2], P('ep'), may hold values from 0 to 3, all different within a row
- gate_weight: bfloat16 [16, 2048, 1024], P('ep', None, 'tp'), may hold values from -0.125 to 0.125
- up_weight: bfloat16 [16, 2048, 1024], P('ep', None, 'tp'), may hold values from -0.125 to 0.125
- down_weight: bfloat16 [16, 1024, 2048], P('ep', 'tp'), may hold values from -0.1875 to 0.1875
Outputs:
- mix_out: bfloat16 [8192, 2048], P(('ep', 'tp'))
- moe_out: bfloat16 [2048, 2048], P('ep', 'tp')
The draws below stay inside these ranges and needn't reach their ends.
All inputs are finite; a program needn't handle non-finite values.
Results may differ from the reference program's by a relative error of at most 0.011.
Values may be sent and summed in bfloat16 or wider, within the bound.
A program may use at most 64 MiB of HBM per device.

```python
import math
import jax
import jax.numpy as jnp
import numpy as np
from jax import lax

D = 2048
FF = 1024
POOL_DIM = 128
POOL_GROUPS = 8
GROUPS = 4
TOPK = 2
WINDOW_MAX = 16
TOK_MOE = 128
D_POOL = 1024
EXPERTS = 16
EPG = 4
CAP = 32
FF_PART = 512
TOKENS_MIX = 8192
TOKENS_MOE = 2048
N_EP = 16
N_TP = 2


def touch_ends(entries, own_key, smallest, top_value):
    dims = entries.shape
    spot = [jax.random.randint(jax.random.fold_in(own_key, axis), (), 0, dims[axis]) for axis in range(len(dims))]
    entries = entries.at[tuple(spot)].set(smallest)
    longest = dims.index(max(dims))
    spot[longest] = (spot[longest] + 1) % dims[longest]
    return entries.at[tuple(spot)].set(top_value)


def shard_levels(stream_key, shape, cuts, smallest, largest):
    factor_of = 1.0
    for dim, parts in cuts:
        steps = jax.random.uniform(jax.random.fold_in(jax.random.fold_in(stream_key, 6), dim), (parts,), jnp.float32, smallest / len(cuts), largest / len(cuts))
        factor_of = factor_of * jnp.repeat(jnp.exp(steps), shape[dim] // parts).reshape((-1,) + (1,) * (len(shape) - 1 - dim))
    return factor_of


def rank_table(count, slope):
    portions = [(1 << 20) // math.isqrt(grade ** slope) + 1 for grade in range(1, count + 1)]
    deviation = 1 + sum(portions) // (1 << 30)
    return np.cumsum(np.array([max(1, weight // deviation) for weight in portions]))


def skewed_ids(stream_key, dims, amount, skew):
    table = rank_table(amount, skew)
    pick = jax.random.randint(jax.random.fold_in(stream_key, 1), dims, 0, int(table[amount - 1]))
    rank = jnp.searchsorted(jnp.asarray(table, jnp.int32), pick, side="right")
    return jax.random.permutation(jax.random.fold_in(stream_key, 2), amount)[rank].astype(jnp.int32)


def distinct(stream_key, rows, amount, top, lift):
    order = jax.random.permutation(jax.random.fold_in(stream_key, 1), amount)
    favour = order
    for power in range(3):
        favour = favour * favour // amount
    favour = favour * lift // amount
    lots = jax.random.randint(jax.random.fold_in(stream_key, 2), (rows, amount), 0, 4096) + favour
    fixed_rows = jax.random.permutation(jax.random.fold_in(stream_key, 3), rows)[jnp.arange(amount) % rows]
    lots = jnp.where(jnp.arange(rows)[:, None] == fixed_rows[None, :], 1 << 14, lots)
    score = lots * amount + jnp.arange(amount)
    return lax.top_k(score.astype(jnp.int32), top)[1].astype(jnp.int32)


def gaussian(own_key, shape, scale, limit, shards=(), held_as=jnp.bfloat16):
    entries = scale * jax.random.normal(own_key, shape, jnp.float32)
    if shards:
        entries = entries * shard_levels(own_key, shape, shards, -0.22, 0.18)
    return jnp.clip(entries, -limit, limit).astype(held_as)


def setup_inputs(seed: int = 0) -> dict:
    keys = jax.random.split(jax.random.key(seed), 14)
    mix_input = gaussian(keys[0], (TOKENS_MIX, D_POOL), 1.0, 6.0, ((0, 32),))
    pool_weight = gaussian(keys[1], (POOL_GROUPS, POOL_DIM, POOL_DIM), POOL_DIM ** -0.5, 0.5)
    pool_scale = jnp.clip(1.0 + 0.18 * jax.random.normal(keys[2], (D_POOL,), jnp.float32), 0.1, 1.9)
    out_weight = gaussian(keys[3], (D_POOL, D), D_POOL ** -0.5, 0.1875)
    moe_input = gaussian(keys[4], (TOKENS_MOE, D), 1.0, 6.0, ((0, 16),))
    moe_gain = jnp.clip(1.0 + 0.18 * jax.random.normal(keys[5], (D,), jnp.float32), 0.1, 1.9)
    group_router = gaussian(keys[6], (D, GROUPS), D ** -0.5, 0.125)
    inner_router = gaussian(keys[7], (D, EXPERTS), D ** -0.5, 0.125)
    group_pick = touch_ends(skewed_ids(keys[8], (TOKENS_MOE,), GROUPS, 2), jax.random.fold_in(keys[8], 3), 0, GROUPS - 1).astype(jnp.int32)
    inner_pick = distinct(keys[9], TOKENS_MOE, EPG, TOPK, 4096)
    gate_weight = gaussian(keys[10], (EXPERTS, D, FF), D ** -0.5, 0.125, ((0, 16), (2, 2)))
    up_weight = gaussian(keys[11], (EXPERTS, D, FF), D ** -0.5, 0.125, ((0, 16), (2, 2)))
    down_weight = gaussian(keys[12], (EXPERTS, FF, D), FF ** -0.5, 0.1875, ((0, 16), (1, 2)))
    return {"mix_input": mix_input, "pool_weight": pool_weight, "pool_scale": pool_scale, "out_weight": out_weight, "moe_input": moe_input, "moe_gain": moe_gain, "group_router": group_router, "inner_router": inner_router, "group_pick": group_pick, "inner_pick": inner_pick, "gate_weight": gate_weight, "up_weight": up_weight, "down_weight": down_weight}


NORM_FLOOR = 0.25

def trailing_means(padded, row_count, lead_rows):
    group_width = padded.shape[1] // 4
    position = jnp.arange(row_count, dtype=jnp.int32)
    pieces = []
    for scale_index in range(4):
        window = 2 ** (scale_index + 1)
        channel_block = padded[:, scale_index * group_width:(scale_index + 1) * group_width]
        window_sum = channel_block[lead_rows:lead_rows + row_count]
        for back_step in range(1, window):
            window_sum = window_sum + channel_block[lead_rows - back_step:lead_rows - back_step + row_count]
        divisor = jnp.minimum(position + 1, window).astype(jnp.float32)
        pieces.append(window_sum / divisor[:, None])
    return jnp.concatenate(pieces, axis=1)

def route_terms(group_logits, inner_logits, group_pick, inner_pick, per_group):
    group_ids = jnp.arange(group_logits.shape[1], dtype=jnp.int32)
    chosen = lax.optimization_barrier(jnp.sum(jnp.where(group_pick[:, None] == group_ids[None, :], group_logits, 0.0), axis=1))
    group_share = 1.0 / lax.optimization_barrier(jnp.sum(jnp.exp(group_logits - chosen[:, None]), axis=1))
    target = (group_pick[:, None] * per_group + inner_pick).astype(jnp.int32)
    expert_ids = jnp.arange(inner_logits.shape[1], dtype=jnp.int32)
    picked = lax.optimization_barrier(jnp.sum(jnp.where(target[:, :, None] == expert_ids[None, None, :], inner_logits[:, None, :], 0.0), axis=2))
    first_share = jax.nn.sigmoid(picked[:, 0] - picked[:, 1])
    route_weight = group_share[:, None] * jnp.stack([first_share, 1.0 - first_share], axis=1)
    return (target, route_weight)

def slot_terms(target, expert_count, capacity):
    expert_ids = jnp.arange(expert_count, dtype=jnp.int32)
    expert_hits = (target[:, :, None] == expert_ids[None, None, :]).astype(jnp.int32)
    per_token = lax.optimization_barrier(jnp.sum(expert_hits, axis=1))
    earlier = jnp.cumsum(per_token, axis=0) - per_token
    route_rank = lax.optimization_barrier(jnp.sum(expert_hits * earlier[:, None, :], axis=2))
    is_kept = route_rank < capacity
    slot_index = (target * capacity + jnp.minimum(route_rank, capacity - 1)).astype(jnp.int32)
    return (slot_index, is_kept)

def slot_sources(slot_index, is_kept, slot_count):
    token_ids = jnp.broadcast_to(jnp.arange(slot_index.shape[0], dtype=jnp.int32)[:, None], slot_index.shape)
    placed = jnp.where(is_kept, slot_index, slot_count).astype(jnp.int32).reshape(-1)
    source = jnp.zeros((slot_count,), jnp.int32).at[placed].set(token_ids.reshape(-1), mode='drop')
    slot_used = jnp.zeros((slot_count,), jnp.bool_).at[placed].set(True, mode='drop')
    return (source, slot_used)

def reference(mix_input, pool_weight, pool_scale, out_weight, moe_input, moe_gain, group_router, inner_router, group_pick, inner_pick, gate_weight, up_weight, down_weight):
    reach_back = WINDOW_MAX - 1
    row_count = mix_input.shape[0]
    values = mix_input.astype(jnp.float32)
    padded = jnp.concatenate([jnp.zeros((reach_back, values.shape[1]), jnp.float32), values], axis=0)
    trailing = trailing_means(padded, row_count, reach_back) - values
    pooled = trailing.astype(jnp.bfloat16)
    grouped = jnp.einsum('tgc,gcd->tgd', pooled.reshape(row_count, POOL_GROUPS, POOL_DIM).astype(jnp.float32), pool_weight.astype(jnp.float32))
    grouped = (grouped.reshape(row_count, D_POOL) * pool_scale[None, :]).astype(jnp.bfloat16)
    mix_out = jnp.dot(grouped, out_weight, preferred_element_type=jnp.float32).astype(jnp.bfloat16)
    token_values = moe_input.astype(jnp.float32)
    norm_scale = lax.rsqrt(jnp.maximum(lax.optimization_barrier(jnp.mean(token_values * token_values, axis=1, keepdims=True)), NORM_FLOOR))
    normed = (token_values * norm_scale * moe_gain[None, :]).astype(jnp.bfloat16)
    group_logits = jnp.dot(normed, group_router, preferred_element_type=jnp.float32)
    inner_logits = jnp.dot(normed, inner_router, preferred_element_type=jnp.float32)
    target, route_weight = route_terms(group_logits, inner_logits, group_pick, inner_pick, EPG)
    block_target = target.reshape(N_EP, TOK_MOE, TOPK)

    def block_slots(one_block):
        return slot_terms(one_block, EXPERTS, CAP)
    slot_index, is_kept = lax.map(block_slots, block_target)

    def block_sources(pair):
        return slot_sources(pair[0], pair[1], EXPERTS * CAP)
    source, slot_used = lax.map(block_sources, (slot_index, is_kept))
    global_source = source + (jnp.arange(N_EP, dtype=jnp.int32) * TOK_MOE)[:, None]
    by_expert = global_source.reshape(N_EP, EXPERTS, CAP).transpose(1, 0, 2).reshape(EXPERTS, N_EP * CAP)
    used_by_expert = slot_used.reshape(N_EP, EXPERTS, CAP).transpose(1, 0, 2).reshape(EXPERTS, N_EP * CAP)

    def run_expert(items):
        token_rows, row_used, gate_matrix, up_matrix, down_matrix = items
        expert_rows = jnp.where(row_used[:, None], normed[token_rows], jnp.zeros((), jnp.bfloat16))
        gate_sum = jnp.dot(expert_rows, gate_matrix, preferred_element_type=jnp.float32)
        up_sum = jnp.dot(expert_rows, up_matrix, preferred_element_type=jnp.float32)
        hidden = (jax.nn.silu(gate_sum) * up_sum).astype(jnp.bfloat16)
        result_sum = jnp.zeros((expert_rows.shape[0], D), jnp.float32)
        for part_index in range(N_TP):
            part_product = jnp.dot(hidden[:, part_index * FF_PART:(part_index + 1) * FF_PART], down_matrix[part_index * FF_PART:(part_index + 1) * FF_PART], preferred_element_type=jnp.float32).astype(jnp.bfloat16)
            result_sum = result_sum + lax.optimization_barrier(part_product).astype(jnp.float32)
        return result_sum.astype(jnp.bfloat16)
    results = lax.map(run_expert, (by_expert, used_by_expert, gate_weight, up_weight, down_weight))
    results = results.reshape(EXPERTS, N_EP, CAP, D)
    flat_slot = slot_index.reshape(TOKENS_MOE, TOPK)
    flat_kept = is_kept.reshape(TOKENS_MOE, TOPK)
    rank_of = (flat_slot - target * CAP).astype(jnp.int32)
    block_of = (jnp.arange(TOKENS_MOE, dtype=jnp.int32) // TOK_MOE)[:, None]
    picked = results[target, block_of, rank_of]
    route_scale = jnp.where(flat_kept, route_weight, 0.0).astype(jnp.bfloat16)
    route_scale = lax.optimization_barrier(route_scale).astype(jnp.float32)
    moe_out = lax.optimization_barrier(jnp.sum(picked.astype(jnp.float32) * route_scale[:, :, None], axis=1)).astype(jnp.bfloat16)
    return (mix_out, moe_out)
```

```python
import functools

import jax
import jax.numpy as jnp
from jax import lax
from jax.experimental import pallas as pl
from jax.experimental.pallas import tpu as pltpu
from jax.sharding import PartitionSpec as P

MESH = pl.DeviceIdType.MESH
CHUNK = 4
LEAD = 16

WINDOW_MAX = 16


NORM_FLOOR = 0.25


def passed_along(value, axis, steps):
    count = lax.axis_size(axis)
    first, last = (max(0, -steps), min(count, count - steps))
    return lax.ppermute(value, axis, [(source, source + steps) for source in range(first, last)])


def trailing_means(extended, row_count, lead_rows, first_position):
    group_width = extended.shape[1] // 4
    position = first_position + jnp.arange(row_count, dtype=jnp.int32)
    pieces = []
    for scale_index in range(4):
        window = 2 ** (scale_index + 1)
        channel_block = extended[:, scale_index * group_width : (scale_index + 1) * group_width]
        window_sum = channel_block[lead_rows : lead_rows + row_count]
        for back_step in range(1, window):
            window_sum = (
                window_sum
                + channel_block[lead_rows - back_step : lead_rows - back_step + row_count]
            )
        divisor = jnp.minimum(position + 1, window).astype(jnp.float32)
        pieces.append(window_sum / divisor[:, None])
    return jnp.concatenate(pieces, axis=1)


def route_terms(group_logits, inner_logits, group_pick, inner_pick, per_group):
    group_ids = jnp.arange(group_logits.shape[1], dtype=jnp.int32)
    chosen = jnp.sum(
        jnp.where(group_pick[:, None] == group_ids[None, :], group_logits, 0.0), axis=1
    )
    group_share = 1.0 / jnp.sum(jnp.exp(group_logits - chosen[:, None]), axis=1)
    target = group_pick[:, None] * per_group + inner_pick
    expert_ids = jnp.arange(inner_logits.shape[1], dtype=jnp.int32)
    picked = jnp.sum(
        jnp.where(target[:, :, None] == expert_ids[None, None, :], inner_logits[:, None, :], 0.0),
        axis=2,
    )
    first_share = jax.nn.sigmoid(picked[:, 0] - picked[:, 1])
    route_weight = group_share[:, None] * jnp.stack([first_share, 1.0 - first_share], axis=1)
    return (target, route_weight)


def slot_terms(target, expert_count, capacity):
    expert_ids = jnp.arange(expert_count, dtype=jnp.int32)
    expert_hits = (target[:, :, None] == expert_ids[None, None, :]).astype(jnp.int32)
    per_token = jnp.sum(expert_hits, axis=1)
    earlier = jnp.cumsum(per_token, axis=0) - per_token
    route_rank = jnp.sum(expert_hits * earlier[:, None, :], axis=2)
    is_kept = route_rank < capacity
    slot_index = target * capacity + jnp.minimum(route_rank, capacity - 1)
    return (slot_index, is_kept)


def slot_sources(slot_index, is_kept, slot_count):
    token_ids = jnp.broadcast_to(
        jnp.arange(slot_index.shape[0], dtype=jnp.int32)[:, None], slot_index.shape
    )
    placed = jnp.where(is_kept, slot_index, slot_count).reshape(-1)
    source = jnp.zeros((slot_count,), jnp.int32).at[placed].set(token_ids.reshape(-1), mode="drop")
    slot_used = jnp.zeros((slot_count,), jnp.bool_).at[placed].set(True, mode="drop")
    return (source, slot_used)


def per_device(
    mix_input,
    pool_weight,
    pool_scale,
    out_weight,
    moe_input,
    moe_gain,
    group_router,
    inner_router,
    group_pick,
    inner_pick,
    gate_weight,
    up_weight,
    down_weight,
):
    row_count = mix_input.shape[0]
    reach_back = WINDOW_MAX - 1
    before = passed_along(mix_input[row_count - reach_back :], ("ep", "tp"), 1)
    extended = jnp.concatenate([before, mix_input], axis=0).astype(jnp.float32)
    first_position = lax.axis_index(("ep", "tp")) * row_count
    trailing = (
        trailing_means(extended, row_count, reach_back, first_position) - extended[reach_back:]
    )
    pooled = trailing.astype(jnp.bfloat16)
    groups, group_dim = (pool_weight.shape[0], pool_weight.shape[1])
    grouped = jnp.einsum(
        "tgc,gcd->tgd",
        pooled.reshape(row_count, groups, group_dim),
        pool_weight,
        preferred_element_type=jnp.float32,
    )
    grouped = (grouped.reshape(row_count, groups * group_dim) * pool_scale[None, :]).astype(
        jnp.bfloat16
    )
    mix_out = jnp.dot(grouped, out_weight, preferred_element_type=jnp.float32).astype(jnp.bfloat16)
    tokens, feature_width = moe_input.shape
    token_values = moe_input.astype(jnp.float32)
    norm_scale = lax.rsqrt(
        jnp.maximum(jnp.mean(token_values * token_values, axis=1, keepdims=True), NORM_FLOOR)
    )
    normed = (token_values * norm_scale * moe_gain[None, :]).astype(jnp.bfloat16)
    group_logits = jnp.dot(normed, group_router, preferred_element_type=jnp.float32)
    inner_logits = jnp.dot(normed, inner_router, preferred_element_type=jnp.float32)
    group_count = group_router.shape[1]
    expert_count = inner_router.shape[1]
    target, route_weight = route_terms(
        group_logits, inner_logits, group_pick, inner_pick, expert_count // group_count
    )
    capacity = 2 * inner_pick.shape[1] * tokens // expert_count
    slot_index, is_kept = slot_terms(target, expert_count, capacity)
    source, slot_used = slot_sources(slot_index, is_kept, expert_count * capacity)
    gate_local = gate_weight[0]
    up_local = up_weight[0]
    outgoing = jnp.where(slot_used[:, None], normed[source], jnp.zeros((), jnp.bfloat16))
    arrived = lax.all_to_all(outgoing, "ep", split_axis=0, concat_axis=0, tiled=True)
    gate_sum = jnp.dot(arrived, gate_local, preferred_element_type=jnp.float32)
    up_sum = jnp.dot(arrived, up_local, preferred_element_type=jnp.float32)
    hidden = (jax.nn.silu(gate_sum) * up_sum).astype(jnp.bfloat16)
    down_local = down_weight[0]
    expert_result = lax.psum_scatter(
        lax.dot_general(
            down_local, hidden, (((0,), (1,)), ((), ())), preferred_element_type=jnp.float32
        ).astype(jnp.bfloat16),
        "tp",
        scatter_dimension=0,
        tiled=True,
    )
    returned = lax.all_to_all(expert_result, "ep", split_axis=1, concat_axis=1, tiled=True)
    route_scale = jnp.where(is_kept, route_weight, 0.0).astype(jnp.bfloat16)
    route_scale = lax.optimization_barrier(route_scale).astype(jnp.float32)
    picked = jnp.take(returned, slot_index, axis=1).astype(jnp.float32)
    combined = jnp.sum(picked * route_scale[None, :, :], axis=2)
    moe_out = combined.T.astype(jnp.bfloat16)
    return (mix_out, moe_out)


def flipped(index, mask, count):
    total = 0
    bit = 1
    while bit < count:
        own = (index // bit) % 2
        total = total + bit * ((1 - own) if mask & bit else own)
        bit *= 2
    return total


def fused_kernel(
    n,
    capacity,
    per_group,
    mix_ref,
    pool_w_ref,
    pool_s_ref,
    out_w_hbm,
    moe_ref,
    gain_ref,
    group_rt_ref,
    inner_rt_ref,
    gp_ref,
    ip_ref,
    gate_hbm,
    up_hbm,
    down_hbm,
    mix_out_ref,
    moe_out_ref,
    out_w,
    gate_w,
    up_w,
    down_w,
    halo,
    pooled_v,
    grouped_v,
    normed_v,
    outgoing,
    arrived,
    part_own,
    part_send,
    part_recv,
    result,
    returned,
    combine_w,
    load_sem,
    halo_sem,
    send_sem,
    recv_sem,
    swap_send,
    swap_recv,
    part_ssem,
    part_rsem,
    ret_send,
    ret_recv,
):
    ep, tp = lax.axis_index("ep"), lax.axis_index("tp")
    other = 1 - tp
    total_devices = 2 * n
    linear = ep * 2 + tp
    following = lax.rem(linear + 1, total_devices)
    preceding = lax.rem(linear + total_devices - 1, total_devices)
    tokens, width = moe_ref.shape
    half = width // 2
    rows = mix_ref.shape[0]
    slots = n * capacity
    near = n // 2
    low, high = (ep // CHUNK) % 2, (ep // near) % 2
    inner = low + high - 2 * low * high

    barrier = pltpu.get_barrier_semaphore()
    greeted = [(flipped(ep, j, n), tp) for j in range(1, n)]
    greeted += [(ep, other), (following // 2, following % 2), (preceding // 2, preceding % 2)]
    for device in greeted:
        pl.semaphore_signal(barrier, inc=1, device_id=device, device_id_type=MESH)

    loads = [
        pltpu.make_async_copy(gate_hbm.at[0], gate_w, load_sem.at[0]),
        pltpu.make_async_copy(up_hbm.at[0], up_w, load_sem.at[1]),
        pltpu.make_async_copy(out_w_hbm, out_w, load_sem.at[2]),
        pltpu.make_async_copy(down_hbm.at[0, :, pl.ds(0, half)], down_w.at[0], load_sem.at[3]),
        pltpu.make_async_copy(down_hbm.at[0, :, pl.ds(half, half)], down_w.at[1], load_sem.at[4]),
    ]
    for index in (0, 1, 3, 4, 2):
        loads[index].start()

    values = moe_ref[...].astype(jnp.float32)
    scale = lax.rsqrt(
        jnp.maximum(jnp.sum(values * values, axis=1, keepdims=True) * (1.0 / width), NORM_FLOOR)
    )
    normed = (values * scale * gain_ref[...]).astype(jnp.bfloat16)
    normed_v[...] = normed

    group_pick = gp_ref[...]
    expert_count = inner_rt_ref.shape[0]
    targets = [group_pick * per_group + ip_ref[k : k + 1, :] for k in range(2)]
    expert_ids = lax.broadcasted_iota(jnp.int32, (expert_count, tokens), 0)
    hits = [expert_ids == target for target in targets]
    both = (hits[0].astype(jnp.float32) + hits[1].astype(jnp.float32)).astype(jnp.bfloat16)
    earlier_mask = (
        lax.broadcasted_iota(jnp.int32, (tokens, tokens), 0)
        < lax.broadcasted_iota(jnp.int32, (tokens, tokens), 1)
    ).astype(jnp.float32).astype(jnp.bfloat16)
    earlier = jnp.dot(both, earlier_mask, preferred_element_type=jnp.float32)
    slot_of = []
    for k in range(2):
        rank = jnp.sum(jnp.where(hits[k], earlier, 0.0), axis=0, keepdims=True).astype(jnp.int32)
        slot_of.append(jnp.where(rank < capacity, targets[k] * capacity + rank, -1))
    slot_ids = lax.broadcasted_iota(jnp.int32, (slots, tokens), 0)
    chosen = [slot_ids == slot for slot in slot_of]
    pick = jnp.where(chosen[0] | chosen[1], 1.0, 0.0).astype(jnp.bfloat16)
    for part in range(2):
        outgoing[part] = jnp.dot(
            pick, normed_v[:, part * half : (part + 1) * half], preferred_element_type=jnp.float32
        ).astype(jnp.bfloat16)

    pl.semaphore_wait(barrier, len(greeted))

    own_rows = pl.ds(pl.multiple_of(ep * capacity, capacity), capacity)
    halo_copy = pltpu.make_async_remote_copy(
        src_ref=mix_ref.at[pl.ds(rows - LEAD, LEAD)],
        dst_ref=halo,
        send_sem=halo_sem.at[0],
        recv_sem=halo_sem.at[1],
        device_id=(following // 2, following % 2),
        device_id_type=MESH,
    )
    halo_copy.start()

    def rows_of(index):
        return pl.ds(pl.multiple_of(index * capacity, capacity), capacity)

    def partner(k):
        there = flipped(ep, k, n)
        if k < near:
            return k, there
        shift = CHUNK if k < near + CHUNK else -CHUNK
        return k + inner * shift, there + inner * (CHUNK - 2 * CHUNK * ((there // CHUNK) % 2))

    def dispatch(k):
        j, there = partner(k)
        if k < near:
            src, dst = outgoing.at[:, rows_of(there)], arrived.at[:, own_rows]
        else:
            src, dst = outgoing.at[tp, rows_of(there)], arrived.at[tp, own_rows]
        return pltpu.make_async_remote_copy(
            src_ref=src,
            dst_ref=dst,
            send_sem=send_sem.at[j],
            recv_sem=recv_sem.at[j],
            device_id=(there, tp),
            device_id_type=MESH,
        )

    def swap(k):
        j, there = partner(k)
        return pltpu.make_async_remote_copy(
            src_ref=arrived.at[tp, rows_of(there)],
            dst_ref=arrived.at[tp, rows_of(there)],
            send_sem=swap_send.at[j],
            recv_sem=swap_recv.at[j],
            device_id=(ep, other),
            device_id_type=MESH,
        )

    def partial_copy(k):
        j, there = partner(k)
        return pltpu.make_async_remote_copy(
            src_ref=part_send.at[rows_of(there)],
            dst_ref=part_recv.at[rows_of(there)],
            send_sem=part_ssem.at[j],
            recv_sem=part_rsem.at[j],
            device_id=(ep, other),
            device_id_type=MESH,
        )

    def give_back(k):
        j, there = partner(k)
        return pltpu.make_async_remote_copy(
            src_ref=result.at[rows_of(there)],
            dst_ref=returned.at[own_rows],
            send_sem=ret_send.at[j],
            recv_sem=ret_recv.at[j],
            device_id=(there, tp),
            device_id_type=MESH,
        )

    for k in range(1, n):
        dispatch(k).start()
    arrived[:, own_rows] = outgoing[:, own_rows]

    def contract(left, right):
        return lax.dot_general(
            left, right, (((1,), (1,)), ((), ())), preferred_element_type=jnp.float32
        )

    group_logits = contract(group_rt_ref[...], normed_v[...])
    inner_logits = contract(inner_rt_ref[...], normed_v[...])
    group_ids = lax.broadcasted_iota(jnp.int32, group_logits.shape, 0)
    own_logit = jnp.sum(
        jnp.where(group_ids == group_pick, group_logits, 0.0), axis=0, keepdims=True
    )
    share = 1.0 / jnp.sum(jnp.exp(group_logits - own_logit), axis=0, keepdims=True)
    picked = [
        jnp.sum(jnp.where(hit, inner_logits, 0.0), axis=0, keepdims=True) for hit in hits
    ]
    first = jax.nn.sigmoid(picked[0] - picked[1])
    weights = [
        (share * value).astype(jnp.bfloat16).astype(jnp.float32) for value in (first, 1.0 - first)
    ]
    spread = jnp.where(chosen[0], weights[0], 0.0) + jnp.where(chosen[1], weights[1], 0.0)
    combine_w[...] = spread.T.astype(jnp.bfloat16)

    def mixer():
        halo_copy.wait()
        group_width = mix_ref.shape[1] // 4
        position = linear * rows + lax.broadcasted_iota(jnp.int32, (rows, 1), 0)
        is_first = linear == 0
        for index in range(4):
            window = 2 ** (index + 1)
            lanes = slice(index * group_width, (index + 1) * group_width)
            lead = jnp.where(is_first, 0.0, halo[:, lanes].astype(jnp.float32))
            body = mix_ref[:, lanes].astype(jnp.float32)
            sums = jnp.concatenate([lead, body], axis=0)
            shift = 1
            while shift < window:
                sums = sums + pltpu.roll(sums, shift, 0)
                shift *= 2
            inverse = 1.0 / jnp.minimum(position + 1, window).astype(jnp.float32)
            pooled_v[:, lanes] = (sums[LEAD:] * inverse - body).astype(jnp.bfloat16)
        group_dim = pool_w_ref.shape[1]
        for g in range(pool_w_ref.shape[0]):
            lanes = slice(g * group_dim, (g + 1) * group_dim)
            product = jnp.dot(pooled_v[:, lanes], pool_w_ref[g], preferred_element_type=jnp.float32)
            grouped_v[:, lanes] = (product * pool_s_ref[:, lanes]).astype(jnp.bfloat16)
        loads[2].wait()
        tile = 512

        @pl.loop(0, mix_out_ref.shape[1] // tile)
        def _(step):
            lanes = pl.ds(pl.multiple_of(step * tile, tile), tile)
            mix_out_ref[:, lanes] = jnp.dot(
                grouped_v[...], out_w[:, lanes], preferred_element_type=jnp.float32
            ).astype(jnp.bfloat16)

    groups = [list(range(first, first + CHUNK)) for first in range(0, n, CHUNK)]

    def expert(group):
        size = len(group)
        start = partner(group[0])[1] // size * (size * capacity)
        span = pl.ds(pl.multiple_of(start, size * capacity), size * capacity)
        sums = []
        for weight in (gate_w, up_w):
            sums.append(
                jnp.dot(arrived[0, span], weight[:half], preferred_element_type=jnp.float32)
                + jnp.dot(arrived[1, span], weight[half:], preferred_element_type=jnp.float32)
            )
        hidden = (sums[0] / (1.0 + jnp.exp(-sums[0])) * sums[1]).astype(jnp.bfloat16)

        def part(index):
            return jnp.dot(
                hidden, down_w[index], preferred_element_type=jnp.float32
            ).astype(jnp.bfloat16)

        part_send[span] = part(other)
        for k in group:
            partial_copy(k).start()
        part_own[span] = part(tp)

    def finish(k):
        block = rows_of(partner(k)[1])
        partial_copy(k).wait_recv()
        total = (
            part_own[block].astype(jnp.float32) + part_recv[block].astype(jnp.float32)
        ).astype(jnp.bfloat16)
        if k == 0:
            returned[block] = total
        else:
            result[block] = total
            give_back(k).start()

    def pass_on(k):
        dispatch(k).wait_recv()
        swap(k).start()

    own, beside, far, last = groups
    early, late = own[:2], own[2:]

    def late_plane():
        for k in late:
            dispatch(k).wait_recv()
        expert(late)

    def late_back():
        for k in late:
            finish(k)

    for index in (0, 1, 3, 4):
        loads[index].wait()
    dispatch(1).wait_recv()
    expert(early)
    mixer()
    pl.when(inner == 0)(late_plane)
    for k in far:
        pass_on(k)
    for k in early:
        finish(k)
    pl.when(inner == 0)(late_back)
    for pair in (far[:2], far[2:]):
        for k in pair:
            swap(k).wait_recv()
        expert(pair)
    for pair in (beside[:2], beside[2:]):
        for k in pair:
            dispatch(k).wait_recv()
        expert(pair)
    for k, earlier_k in zip(last, far):
        pass_on(k)
        finish(earlier_k)
    for k in beside:
        finish(k)
    for pair in (last[:2], last[2:]):
        for k in pair:
            swap(k).wait_recv()
        expert(pair)
    pl.when(inner == 1)(late_plane)
    for k in last:
        finish(k)
    pl.when(inner == 1)(late_back)
    for k in far:
        give_back(k).wait_recv()
    for k in beside:
        give_back(k).wait_recv()
    for k in last:
        give_back(k).wait_recv()
    for k in own[1:]:
        give_back(k).wait_recv()
    moe_out_ref[...] = jnp.dot(
        combine_w[...], returned[...], preferred_element_type=jnp.float32
    ).astype(jnp.bfloat16)
    partial_copy(0).wait_send()
    for k in range(1, n):
        dispatch(k).wait_send()
        give_back(k).wait_send()
        partial_copy(k).wait_send()
        if k >= near:
            swap(k).wait_send()


def fused(
    mix_input,
    pool_weight,
    pool_scale,
    out_weight,
    moe_input,
    moe_gain,
    group_router,
    inner_router,
    group_pick,
    inner_pick,
    gate_weight,
    up_weight,
    down_weight,
):
    n = lax.axis_size("ep")
    tokens, width = moe_input.shape
    rows, channels = mix_input.shape
    expert_count = inner_router.shape[1]
    capacity = 2 * inner_pick.shape[1] * tokens // expert_count
    half = width // 2
    slots = n * capacity
    hidden = gate_weight.shape[2]
    bf16 = jnp.bfloat16
    vmem = pl.BlockSpec(memory_space=pltpu.VMEM)
    hbm = pl.BlockSpec(memory_space=pl.ANY)
    dma = pltpu.SemaphoreType.DMA
    return pl.pallas_call(
        functools.partial(
            fused_kernel, n, capacity, expert_count // group_router.shape[1]
        ),
        out_shape=(
            pltpu.VMEM((rows, out_weight.shape[1]), bf16),
            pltpu.VMEM((tokens, half), bf16),
        ),
        in_specs=[vmem, vmem, vmem, hbm] + [vmem] * 6 + [hbm] * 3,
        out_specs=(vmem, vmem),
        scratch_shapes=[
            pltpu.VMEM(out_weight.shape, bf16),
            pltpu.VMEM((width, hidden), bf16),
            pltpu.VMEM((width, hidden), bf16),
            pltpu.VMEM((2, hidden, half), bf16),
            pltpu.VMEM((LEAD, channels), bf16),
            pltpu.VMEM((rows, channels), bf16),
            pltpu.VMEM((rows, channels), bf16),
            pltpu.VMEM((tokens, width), bf16),
            pltpu.VMEM((2, slots, half), bf16),
            pltpu.VMEM((2, slots, half), bf16),
            pltpu.VMEM((slots, half), bf16),
            pltpu.VMEM((slots, half), bf16),
            pltpu.VMEM((slots, half), bf16),
            pltpu.VMEM((slots, half), bf16),
            pltpu.VMEM((slots, half), bf16),
            pltpu.VMEM((tokens, slots), bf16),
            dma((5,)),
            dma((2,)),
            dma((n,)),
            dma((n,)),
            dma((n,)),
            dma((n,)),
            dma((n,)),
            dma((n,)),
            dma((n,)),
            dma((n,)),
        ],
        compiler_params=pltpu.CompilerParams(
            collective_id=0, has_side_effects=True, vmem_limit_bytes=60 * 1024 * 1024
        ),
    )(
        mix_input,
        pool_weight,
        pool_scale[None, :],
        out_weight,
        moe_input,
        moe_gain[None, :],
        group_router.T,
        inner_router.T,
        group_pick[None, :],
        inner_pick.T,
        gate_weight,
        up_weight,
        down_weight,
    )


def step(*arrays):
    mix_input, moe_input, inner_router, inner_pick = arrays[0], arrays[4], arrays[7], arrays[9]
    n, n_tp = lax.axis_size("ep"), lax.axis_size("tp")
    capacity = 2 * inner_pick.shape[1] * moe_input.shape[0] // inner_router.shape[1]
    fits = (
        n_tp == 2
        and inner_pick.shape[1] == 2
        and n == 4 * CHUNK
        and inner_router.shape[1] == n
        and capacity % 16 == 0
        and mix_input.shape[0] >= LEAD
    )
    return fused(*arrays) if fits else per_device(*arrays)


def solution(mesh):
    in_specs = (
        P(("ep", "tp"), None),
        P(),
        P(),
        P(),
        P("ep", None),
        P(),
        P(),
        P(),
        P("ep"),
        P("ep", None),
        P("ep", None, "tp"),
        P("ep", None, "tp"),
        P("ep", "tp", None),
    )
    out_specs = (P(("ep", "tp"), None), P("ep", "tp"))
    return jax.shard_map(
        step, mesh=mesh, in_specs=in_specs, out_specs=out_specs, check_vma=False
    )
```

```python
import functools

import jax
import jax.numpy as jnp
from jax import lax
from jax.experimental import pallas as pl
from jax.experimental.pallas import tpu as pltpu
from jax.sharding import PartitionSpec as P

MESH = pl.DeviceIdType.MESH
CHUNK = 4
LEAD = 16

WINDOW_MAX = 16


NORM_FLOOR = 0.25


def passed_along(value, axis, steps):
    count = lax.axis_size(axis)
    first, last = (max(0, -steps), min(count, count - steps))
    return lax.ppermute(value, axis, [(source, source + steps) for source in range(first, last)])


def trailing_means(extended, row_count, lead_rows, first_position):
    group_width = extended.shape[1] // 4
    position = first_position + jnp.arange(row_count, dtype=jnp.int32)
    pieces = []
    for scale_index in range(4):
        window = 2 ** (scale_index + 1)
        channel_block = extended[:, scale_index * group_width : (scale_index + 1) * group_width]
        window_sum = channel_block[lead_rows : lead_rows + row_count]
        for back_step in range(1, window):
            window_sum = (
                window_sum
                + channel_block[lead_rows - back_step : lead_rows - back_step + row_count]
            )
        divisor = jnp.minimum(position + 1, window).astype(jnp.float32)
        pieces.append(window_sum / divisor[:, None])
    return jnp.concatenate(pieces, axis=1)


def route_terms(group_logits, inner_logits, group_pick, inner_pick, per_group):
    group_ids = jnp.arange(group_logits.shape[1], dtype=jnp.int32)
    chosen = jnp.sum(
        jnp.where(group_pick[:, None] == group_ids[None, :], group_logits, 0.0), axis=1
    )
    group_share = 1.0 / jnp.sum(jnp.exp(group_logits - chosen[:, None]), axis=1)
    target = group_pick[:, None] * per_group + inner_pick
    expert_ids = jnp.arange(inner_logits.shape[1], dtype=jnp.int32)
    picked = jnp.sum(
        jnp.where(target[:, :, None] == expert_ids[None, None, :], inner_logits[:, None, :], 0.0),
        axis=2,
    )
    first_share = jax.nn.sigmoid(picked[:, 0] - picked[:, 1])
    route_weight = group_share[:, None] * jnp.stack([first_share, 1.0 - first_share], axis=1)
    return (target, route_weight)


def slot_terms(target, expert_count, capacity):
    expert_ids = jnp.arange(expert_count, dtype=jnp.int32)
    expert_hits = (target[:, :, None] == expert_ids[None, None, :]).astype(jnp.int32)
    per_token = jnp.sum(expert_hits, axis=1)
    earlier = jnp.cumsum(per_token, axis=0) - per_token
    route_rank = jnp.sum(expert_hits * earlier[:, None, :], axis=2)
    is_kept = route_rank < capacity
    slot_index = target * capacity + jnp.minimum(route_rank, capacity - 1)
    return (slot_index, is_kept)


def slot_sources(slot_index, is_kept, slot_count):
    token_ids = jnp.broadcast_to(
        jnp.arange(slot_index.shape[0], dtype=jnp.int32)[:, None], slot_index.shape
    )
    placed = jnp.where(is_kept, slot_index, slot_count).reshape(-1)
    source = jnp.zeros((slot_count,), jnp.int32).at[placed].set(token_ids.reshape(-1), mode="drop")
    slot_used = jnp.zeros((slot_count,), jnp.bool_).at[placed].set(True, mode="drop")
    return (source, slot_used)


def per_device(
    mix_input,
    pool_weight,
    pool_scale,
    out_weight,
    moe_input,
    moe_gain,
    group_router,
    inner_router,
    group_pick,
    inner_pick,
    gate_weight,
    up_weight,
    down_weight,
):
    row_count = mix_input.shape[0]
    reach_back = WINDOW_MAX - 1
    before = passed_along(mix_input[row_count - reach_back :], ("ep", "tp"), 1)
    extended = jnp.concatenate([before, mix_input], axis=0).astype(jnp.float32)
    first_position = lax.axis_index(("ep", "tp")) * row_count
    trailing = (
        trailing_means(extended, row_count, reach_back, first_position) - extended[reach_back:]
    )
    pooled = trailing.astype(jnp.bfloat16)
    groups, group_dim = (pool_weight.shape[0], pool_weight.shape[1])
    grouped = jnp.einsum(
        "tgc,gcd->tgd",
        pooled.reshape(row_count, groups, group_dim),
        pool_weight,
        preferred_element_type=jnp.float32,
    )
    grouped = (grouped.reshape(row_count, groups * group_dim) * pool_scale[None, :]).astype(
        jnp.bfloat16
    )
    mix_out = jnp.dot(grouped, out_weight, preferred_element_type=jnp.float32).astype(jnp.bfloat16)
    tokens, feature_width = moe_input.shape
    token_values = moe_input.astype(jnp.float32)
    norm_scale = lax.rsqrt(
        jnp.maximum(jnp.mean(token_values * token_values, axis=1, keepdims=True), NORM_FLOOR)
    )
    normed = (token_values * norm_scale * moe_gain[None, :]).astype(jnp.bfloat16)
    group_logits = jnp.dot(normed, group_router, preferred_element_type=jnp.float32)
    inner_logits = jnp.dot(normed, inner_router, preferred_element_type=jnp.float32)
    group_count = group_router.shape[1]
    expert_count = inner_router.shape[1]
    target, route_weight = route_terms(
        group_logits, inner_logits, group_pick, inner_pick, expert_count // group_count
    )
    capacity = 2 * inner_pick.shape[1] * tokens // expert_count
    slot_index, is_kept = slot_terms(target, expert_count, capacity)
    source, slot_used = slot_sources(slot_index, is_kept, expert_count * capacity)
    gate_local = gate_weight[0]
    up_local = up_weight[0]
    outgoing = jnp.where(slot_used[:, None], normed[source], jnp.zeros((), jnp.bfloat16))
    arrived = lax.all_to_all(outgoing, "ep", split_axis=0, concat_axis=0, tiled=True)
    gate_sum = jnp.dot(arrived, gate_local, preferred_element_type=jnp.float32)
    up_sum = jnp.dot(arrived, up_local, preferred_element_type=jnp.float32)
    hidden = (jax.nn.silu(gate_sum) * up_sum).astype(jnp.bfloat16)
    down_local = down_weight[0]
    expert_result = lax.psum_scatter(
        lax.dot_general(
            down_local, hidden, (((0,), (1,)), ((), ())), preferred_element_type=jnp.float32
        ).astype(jnp.bfloat16),
        "tp",
        scatter_dimension=0,
        tiled=True,
    )
    returned = lax.all_to_all(expert_result, "ep", split_axis=1, concat_axis=1, tiled=True)
    route_scale = jnp.where(is_kept, route_weight, 0.0).astype(jnp.bfloat16)
    route_scale = lax.optimization_barrier(route_scale).astype(jnp.float32)
    picked = jnp.take(returned, slot_index, axis=1).astype(jnp.float32)
    combined = jnp.sum(picked * route_scale[None, :, :], axis=2)
    moe_out = combined.T.astype(jnp.bfloat16)
    return (mix_out, moe_out)


def flipped(index, mask, count):
    total = 0
    bit = 1
    while bit < count:
        own = (index // bit) % 2
        total = total + bit * ((1 - own) if mask & bit else own)
        bit *= 2
    return total


def fused_kernel(
    n,
    capacity,
    per_group,
    mix_ref,
    pool_w_ref,
    pool_s_ref,
    out_w_hbm,
    moe_ref,
    gain_ref,
    group_rt_ref,
    inner_rt_ref,
    gp_ref,
    ip_ref,
    gate_hbm,
    up_hbm,
    down_hbm,
    mix_out_ref,
    moe_out_ref,
    out_w,
    gate_w,
    up_w,
    down_w,
    halo,
    pooled_v,
    grouped_v,
    normed_v,
    outgoing,
    arrived,
    part_own,
    part_send,
    part_recv,
    result,
    returned,
    combine_w,
    slot_info,
    raw_info,
    raw_rows,
    relayed,
    load_sem,
    halo_sem,
    send_sem,
    recv_sem,
    swap_send,
    swap_recv,
    part_ssem,
    part_rsem,
    ret_send,
    ret_recv,
    raw_sem,
    relay_send,
):
    ep, tp = lax.axis_index("ep"), lax.axis_index("tp")
    other = 1 - tp
    total_devices = 2 * n
    linear = ep * 2 + tp
    following = lax.rem(linear + 1, total_devices)
    preceding = lax.rem(linear + total_devices - 1, total_devices)
    tokens, width = moe_ref.shape
    half = width // 2
    rows = mix_ref.shape[0]
    slots = n * capacity
    near = n // 2
    low, high = (ep // CHUNK) % 2, (ep // near) % 2
    inner = low + high - 2 * low * high

    barrier = pltpu.get_barrier_semaphore()
    greeted = [(flipped(ep, j, n), tp) for j in range(1, n)]
    greeted += [(ep, other), (following // 2, following % 2), (preceding // 2, preceding % 2)]
    for device in greeted:
        pl.semaphore_signal(barrier, inc=1, device_id=device, device_id_type=MESH)

    loads = [
        pltpu.make_async_copy(gate_hbm.at[0], gate_w, load_sem.at[0]),
        pltpu.make_async_copy(up_hbm.at[0], up_w, load_sem.at[1]),
        pltpu.make_async_copy(out_w_hbm, out_w, load_sem.at[2]),
        pltpu.make_async_copy(down_hbm.at[0, :, pl.ds(0, half)], down_w.at[0], load_sem.at[3]),
        pltpu.make_async_copy(down_hbm.at[0, :, pl.ds(half, half)], down_w.at[1], load_sem.at[4]),
    ]
    for index in (0, 1, 3, 4, 2):
        loads[index].start()

    values = moe_ref[...].astype(jnp.float32)
    scale = lax.rsqrt(
        jnp.maximum(jnp.sum(values * values, axis=1, keepdims=True) * (1.0 / width), NORM_FLOOR)
    )
    normed = (values * scale * gain_ref[...]).astype(jnp.bfloat16)
    for part in range(2):
        normed_v[part] = normed[:, part * half : (part + 1) * half]

    group_pick = gp_ref[...]
    expert_count = inner_rt_ref.shape[0]
    targets = [group_pick * per_group + ip_ref[k : k + 1, :] for k in range(2)]
    expert_ids = lax.broadcasted_iota(jnp.int32, (expert_count, tokens), 0)
    hits = [expert_ids == target for target in targets]
    both = (hits[0].astype(jnp.float32) + hits[1].astype(jnp.float32)).astype(jnp.bfloat16)
    earlier_mask = (
        lax.broadcasted_iota(jnp.int32, (tokens, tokens), 0)
        < lax.broadcasted_iota(jnp.int32, (tokens, tokens), 1)
    ).astype(jnp.float32).astype(jnp.bfloat16)
    earlier = jnp.dot(both, earlier_mask, preferred_element_type=jnp.float32)
    slot_of = []
    for k in range(2):
        rank = jnp.sum(jnp.where(hits[k], earlier, 0.0), axis=0, keepdims=True).astype(jnp.int32)
        slot_of.append(jnp.where(rank < capacity, targets[k] * capacity + rank, -1))
    slot_ids = lax.broadcasted_iota(jnp.int32, (slots, tokens), 0)
    chosen = [slot_ids == slot for slot in slot_of]
    pick = jnp.where(chosen[0] | chosen[1], 1.0, 0.0).astype(jnp.bfloat16)
    for part in range(2):
        outgoing[part] = jnp.dot(
            pick, normed_v[part], preferred_element_type=jnp.float32
        ).astype(jnp.bfloat16)
    for k in range(2):
        slot_info[k : k + 1, :] = slot_of[k]

    pl.semaphore_wait(barrier, len(greeted))

    own_rows = pl.ds(pl.multiple_of(ep * capacity, capacity), capacity)
    halo_copy = pltpu.make_async_remote_copy(
        src_ref=mix_ref.at[pl.ds(rows - LEAD, LEAD)],
        dst_ref=halo,
        send_sem=halo_sem.at[0],
        recv_sem=halo_sem.at[1],
        device_id=(following // 2, following % 2),
        device_id_type=MESH,
    )
    halo_copy.start()

    relay_lanes = [slice(first, first + half // 2) for first in range(0, half, half // 2)]

    def rows_of(index):
        return pl.ds(pl.multiple_of(index * capacity, capacity), capacity)

    def partner(k):
        there = flipped(ep, k, n)
        if k < near:
            return k, there
        shift = CHUNK if k < near + CHUNK else -CHUNK
        return k + inner * shift, there + inner * (CHUNK - 2 * CHUNK * ((there // CHUNK) % 2))

    def dispatch(k):
        j, there = partner(k)
        if k < near:
            src, dst = outgoing.at[:, rows_of(there)], arrived.at[:, own_rows]
        else:
            src, dst = outgoing.at[tp, rows_of(there)], arrived.at[tp, own_rows]
        return pltpu.make_async_remote_copy(
            src_ref=src,
            dst_ref=dst,
            send_sem=send_sem.at[j],
            recv_sem=recv_sem.at[j],
            device_id=(there, tp),
            device_id_type=MESH,
        )

    def swap(k):
        j, there = partner(k)
        return pltpu.make_async_remote_copy(
            src_ref=arrived.at[tp, rows_of(there)],
            dst_ref=arrived.at[tp, rows_of(there)],
            send_sem=swap_send.at[j],
            recv_sem=swap_recv.at[j],
            device_id=(ep, other),
            device_id_type=MESH,
        )

    def partial_copy(k):
        j, there = partner(k)
        return pltpu.make_async_remote_copy(
            src_ref=part_send.at[rows_of(there)],
            dst_ref=part_recv.at[rows_of(there)],
            send_sem=part_ssem.at[j],
            recv_sem=part_rsem.at[j],
            device_id=(ep, other),
            device_id_type=MESH,
        )

    def give_back(k):
        j, there = partner(k)
        return pltpu.make_async_remote_copy(
            src_ref=result.at[rows_of(there)],
            dst_ref=returned.at[own_rows],
            send_sem=ret_send.at[j],
            recv_sem=ret_recv.at[j],
            device_id=(there, tp),
            device_id_type=MESH,
        )

    raw_copies = [
        pltpu.make_async_remote_copy(
            src_ref=src,
            dst_ref=dst,
            send_sem=raw_sem.at[0, index],
            recv_sem=raw_sem.at[1, index],
            device_id=(flipped(ep, near, n), tp),
            device_id_type=MESH,
        )
        for index, (src, dst) in enumerate(
            [(slot_info, raw_info)]
            + [(normed_v.at[tp, :, lanes], raw_rows.at[:, lanes]) for lanes in relay_lanes]
        )
    ]

    def relay_copy(m, lanes, index):
        there = flipped(ep, m, n)
        return pltpu.make_async_remote_copy(
            src_ref=relayed.at[rows_of(there % near), lanes],
            dst_ref=arrived.at[tp, rows_of(flipped(ep, near, n)), lanes],
            send_sem=relay_send.at[index, m],
            recv_sem=recv_sem.at[near + m],
            device_id=(there, tp),
            device_id_type=MESH,
        )

    relay_order = list(range(CHUNK, near)) + list(range(1, CHUNK))

    def relay():
        raw_copies[0].wait_recv()
        first_slot = (ep // near) * (near * capacity)
        half_ids = lax.broadcasted_iota(jnp.int32, (near * capacity, tokens), 0) + first_slot
        half_pick = jnp.where(
            (half_ids == raw_info[0:1, :]) | (half_ids == raw_info[1:2, :]), 1.0, 0.0
        ).astype(jnp.bfloat16)
        for index, lanes in enumerate(relay_lanes):
            raw_copies[1 + index].wait_recv()
            relayed[:, lanes] = jnp.dot(
                half_pick, raw_rows[:, lanes], preferred_element_type=jnp.float32
            ).astype(jnp.bfloat16)
            for m in relay_order:
                relay_copy(m, lanes, index).start()
            arrived[tp, rows_of(flipped(ep, near, n)), lanes] = relayed[rows_of(ep % near), lanes]

    def sends_outer():
        for copy in raw_copies:
            copy.start()

    def sends_inner():
        for k in range(near, n):
            dispatch(k).start()

    def sent_outer():
        for copy in raw_copies:
            copy.wait_send()

    def sent_inner():
        for k in range(near, n):
            dispatch(k).wait_send()
        for index, lanes in enumerate(relay_lanes):
            for m in relay_order:
                relay_copy(m, lanes, index).wait_send()

    for k in range(1, near):
        dispatch(k).start()
    pl.when(inner == 0)(sends_outer)
    pl.when(inner == 1)(sends_inner)
    arrived[:, own_rows] = outgoing[:, own_rows]

    def contract(left, right):
        return lax.dot_general(
            left, right, (((1,), (1,)), ((), ())), preferred_element_type=jnp.float32
        )

    def logits_of(router):
        return contract(router[:, :half], normed_v[0]) + contract(router[:, half:], normed_v[1])

    group_logits = logits_of(group_rt_ref)
    inner_logits = logits_of(inner_rt_ref)
    group_ids = lax.broadcasted_iota(jnp.int32, group_logits.shape, 0)
    own_logit = jnp.sum(
        jnp.where(group_ids == group_pick, group_logits, 0.0), axis=0, keepdims=True
    )
    share = 1.0 / jnp.sum(jnp.exp(group_logits - own_logit), axis=0, keepdims=True)
    picked = [
        jnp.sum(jnp.where(hit, inner_logits, 0.0), axis=0, keepdims=True) for hit in hits
    ]
    first = jax.nn.sigmoid(picked[0] - picked[1])
    weights = [
        (share * value).astype(jnp.bfloat16).astype(jnp.float32) for value in (first, 1.0 - first)
    ]
    spread = jnp.where(chosen[0], weights[0], 0.0) + jnp.where(chosen[1], weights[1], 0.0)
    combine_w[...] = spread.T.astype(jnp.bfloat16)

    def mixer():
        halo_copy.wait()
        group_width = mix_ref.shape[1] // 4
        position = linear * rows + lax.broadcasted_iota(jnp.int32, (rows, 1), 0)
        is_first = linear == 0
        for index in range(4):
            window = 2 ** (index + 1)
            lanes = slice(index * group_width, (index + 1) * group_width)
            lead = jnp.where(is_first, 0.0, halo[:, lanes].astype(jnp.float32))
            body = mix_ref[:, lanes].astype(jnp.float32)
            sums = jnp.concatenate([lead, body], axis=0)
            shift = 1
            while shift < window:
                sums = sums + pltpu.roll(sums, shift, 0)
                shift *= 2
            inverse = 1.0 / jnp.minimum(position + 1, window).astype(jnp.float32)
            pooled_v[:, lanes] = (sums[LEAD:] * inverse - body).astype(jnp.bfloat16)
        group_dim = pool_w_ref.shape[1]
        for g in range(pool_w_ref.shape[0]):
            lanes = slice(g * group_dim, (g + 1) * group_dim)
            product = jnp.dot(pooled_v[:, lanes], pool_w_ref[g], preferred_element_type=jnp.float32)
            grouped_v[:, lanes] = (product * pool_s_ref[:, lanes]).astype(jnp.bfloat16)
        loads[2].wait()
        tile = 512

        @pl.loop(0, mix_out_ref.shape[1] // tile)
        def _(step):
            lanes = pl.ds(pl.multiple_of(step * tile, tile), tile)
            mix_out_ref[:, lanes] = jnp.dot(
                grouped_v[...], out_w[:, lanes], preferred_element_type=jnp.float32
            ).astype(jnp.bfloat16)

    groups = [list(range(first, first + CHUNK)) for first in range(0, n, CHUNK)]

    def expert(group):
        size = len(group)
        start = partner(group[0])[1] // size * (size * capacity)
        span = pl.ds(pl.multiple_of(start, size * capacity), size * capacity)
        sums = []
        for weight in (gate_w, up_w):
            sums.append(
                jnp.dot(arrived[0, span], weight[:half], preferred_element_type=jnp.float32)
                + jnp.dot(arrived[1, span], weight[half:], preferred_element_type=jnp.float32)
            )
        hidden = (sums[0] / (1.0 + jnp.exp(-sums[0])) * sums[1]).astype(jnp.bfloat16)

        def part(index):
            return jnp.dot(
                hidden, down_w[index], preferred_element_type=jnp.float32
            ).astype(jnp.bfloat16)

        part_send[span] = part(other)
        for k in group:
            partial_copy(k).start()
        part_own[span] = part(tp)

    def finish(k):
        block = rows_of(partner(k)[1])
        partial_copy(k).wait_recv()
        total = (
            part_own[block].astype(jnp.float32) + part_recv[block].astype(jnp.float32)
        ).astype(jnp.bfloat16)
        if k == 0:
            returned[block] = total
        else:
            result[block] = total
            give_back(k).start()

    def pass_on(k):
        if k == near + CHUNK:
            pl.when(inner == 0)(dispatch(k).wait_recv)
        else:
            dispatch(k).wait_recv()
        swap(k).start()

    own, beside, far, last = groups
    early, late = own[:2], own[2:]

    def late_plane():
        for k in late:
            dispatch(k).wait_recv()
        expert(late)

    def late_back():
        for k in late:
            finish(k)

    for index in (0, 1, 3, 4):
        loads[index].wait()
    dispatch(1).wait_recv()
    expert(early)
    mixer()
    pl.when(inner == 0)(late_plane)
    for k in far:
        pass_on(k)
    for k in early:
        finish(k)
    pl.when(inner == 0)(late_back)
    for pair in (far[:2], far[2:]):
        for k in pair:
            swap(k).wait_recv()
        expert(pair)
    for pair in (beside[:2], beside[2:]):
        for k in pair:
            dispatch(k).wait_recv()
        expert(pair)
    for k in far:
        finish(k)
    pl.when(inner == 1)(relay)
    for k in last:
        pass_on(k)
    for k in beside:
        finish(k)
    for pair in (last[:2], last[2:]):
        for k in pair:
            swap(k).wait_recv()
        expert(pair)
    pl.when(inner == 1)(late_plane)
    for k in last:
        finish(k)
    pl.when(inner == 1)(late_back)
    for k in far:
        give_back(k).wait_recv()
    for k in beside:
        give_back(k).wait_recv()
    for k in last:
        give_back(k).wait_recv()
    for k in own[1:]:
        give_back(k).wait_recv()
    moe_out_ref[...] = jnp.dot(
        combine_w[...], returned[...], preferred_element_type=jnp.float32
    ).astype(jnp.bfloat16)
    partial_copy(0).wait_send()
    pl.when(inner == 0)(sent_outer)
    pl.when(inner == 1)(sent_inner)
    for k in range(1, n):
        if k < near:
            dispatch(k).wait_send()
        give_back(k).wait_send()
        partial_copy(k).wait_send()
        if k >= near:
            swap(k).wait_send()


def fused(
    mix_input,
    pool_weight,
    pool_scale,
    out_weight,
    moe_input,
    moe_gain,
    group_router,
    inner_router,
    group_pick,
    inner_pick,
    gate_weight,
    up_weight,
    down_weight,
):
    n = lax.axis_size("ep")
    tokens, width = moe_input.shape
    rows, channels = mix_input.shape
    expert_count = inner_router.shape[1]
    capacity = 2 * inner_pick.shape[1] * tokens // expert_count
    half = width // 2
    slots = n * capacity
    hidden = gate_weight.shape[2]
    bf16 = jnp.bfloat16
    vmem = pl.BlockSpec(memory_space=pltpu.VMEM)
    hbm = pl.BlockSpec(memory_space=pl.ANY)
    dma = pltpu.SemaphoreType.DMA
    return pl.pallas_call(
        functools.partial(
            fused_kernel, n, capacity, expert_count // group_router.shape[1]
        ),
        out_shape=(
            pltpu.VMEM((rows, out_weight.shape[1]), bf16),
            pltpu.VMEM((tokens, half), bf16),
        ),
        in_specs=[vmem, vmem, vmem, hbm] + [vmem] * 6 + [hbm] * 3,
        out_specs=(vmem, vmem),
        scratch_shapes=[
            pltpu.VMEM(out_weight.shape, bf16),
            pltpu.VMEM((width, hidden), bf16),
            pltpu.VMEM((width, hidden), bf16),
            pltpu.VMEM((2, hidden, half), bf16),
            pltpu.VMEM((LEAD, channels), bf16),
            pltpu.VMEM((rows, channels), bf16),
            pltpu.VMEM((rows, channels), bf16),
            pltpu.VMEM((2, tokens, half), bf16),
            pltpu.VMEM((2, slots, half), bf16),
            pltpu.VMEM((2, slots, half), bf16),
            pltpu.VMEM((slots, half), bf16),
            pltpu.VMEM((slots, half), bf16),
            pltpu.VMEM((slots, half), bf16),
            pltpu.VMEM((slots, half), bf16),
            pltpu.VMEM((slots, half), bf16),
            pltpu.VMEM((tokens, slots), bf16),
            pltpu.VMEM((2, tokens), jnp.int32),
            pltpu.VMEM((2, tokens), jnp.int32),
            pltpu.VMEM((tokens, half), bf16),
            pltpu.VMEM((slots // 2, half), bf16),
            dma((5,)),
            dma((2,)),
            dma((n,)),
            dma((n,)),
            dma((n,)),
            dma((n,)),
            dma((n,)),
            dma((n,)),
            dma((n,)),
            dma((n,)),
            dma((2, 3)),
            dma((2, n // 2)),
        ],
        compiler_params=pltpu.CompilerParams(
            collective_id=0, has_side_effects=True, vmem_limit_bytes=60 * 1024 * 1024
        ),
    )(
        mix_input,
        pool_weight,
        pool_scale[None, :],
        out_weight,
        moe_input,
        moe_gain[None, :],
        group_router.T,
        inner_router.T,
        group_pick[None, :],
        inner_pick.T,
        gate_weight,
        up_weight,
        down_weight,
    )


def step(*arrays):
    mix_input, moe_input, inner_router, inner_pick = arrays[0], arrays[4], arrays[7], arrays[9]
    n, n_tp = lax.axis_size("ep"), lax.axis_size("tp")
    capacity = 2 * inner_pick.shape[1] * moe_input.shape[0] // inner_router.shape[1]
    fits = (
        n_tp == 2
        and inner_pick.shape[1] == 2
        and n == 4 * CHUNK
        and inner_router.shape[1] == n
        and capacity % 16 == 0
        and mix_input.shape[0] >= LEAD
    )
    return fused(*arrays) if fits else per_device(*arrays)


def solution(mesh):
    in_specs = (
        P(("ep", "tp"), None),
        P(),
        P(),
        P(),
        P("ep", None),
        P(),
        P(),
        P(),
        P("ep"),
        P("ep", None),
        P("ep", None, "tp"),
        P("ep", None, "tp"),
        P("ep", "tp", None),
    )
    out_specs = (P(("ep", "tp"), None), P("ep", "tp"))
    return jax.shard_map(
        step, mesh=mesh, in_specs=in_specs, out_specs=out_specs, check_vma=False
    )
```

```python
import functools

import jax
import jax.numpy as jnp
from jax import lax
from jax.experimental import pallas as pl
from jax.experimental.pallas import tpu as pltpu
from jax.sharding import PartitionSpec as P

MESH = pl.DeviceIdType.MESH
CHUNK = 4
LEAD = 16

WINDOW_MAX = 16


NORM_FLOOR = 0.25


def passed_along(value, axis, steps):
    count = lax.axis_size(axis)
    first, last = (max(0, -steps), min(count, count - steps))
    return lax.ppermute(value, axis, [(source, source + steps) for source in range(first, last)])


def trailing_means(extended, row_count, lead_rows, first_position):
    group_width = extended.shape[1] // 4
    position = first_position + jnp.arange(row_count, dtype=jnp.int32)
    pieces = []
    for scale_index in range(4):
        window = 2 ** (scale_index + 1)
        channel_block = extended[:, scale_index * group_width : (scale_index + 1) * group_width]
        window_sum = channel_block[lead_rows : lead_rows + row_count]
        for back_step in range(1, window):
            window_sum = (
                window_sum
                + channel_block[lead_rows - back_step : lead_rows - back_step + row_count]
            )
        divisor = jnp.minimum(position + 1, window).astype(jnp.float32)
        pieces.append(window_sum / divisor[:, None])
    return jnp.concatenate(pieces, axis=1)


def route_terms(group_logits, inner_logits, group_pick, inner_pick, per_group):
    group_ids = jnp.arange(group_logits.shape[1], dtype=jnp.int32)
    chosen = jnp.sum(
        jnp.where(group_pick[:, None] == group_ids[None, :], group_logits, 0.0), axis=1
    )
    group_share = 1.0 / jnp.sum(jnp.exp(group_logits - chosen[:, None]), axis=1)
    target = group_pick[:, None] * per_group + inner_pick
    expert_ids = jnp.arange(inner_logits.shape[1], dtype=jnp.int32)
    picked = jnp.sum(
        jnp.where(target[:, :, None] == expert_ids[None, None, :], inner_logits[:, None, :], 0.0),
        axis=2,
    )
    first_share = jax.nn.sigmoid(picked[:, 0] - picked[:, 1])
    route_weight = group_share[:, None] * jnp.stack([first_share, 1.0 - first_share], axis=1)
    return (target, route_weight)


def slot_terms(target, expert_count, capacity):
    expert_ids = jnp.arange(expert_count, dtype=jnp.int32)
    expert_hits = (target[:, :, None] == expert_ids[None, None, :]).astype(jnp.int32)
    per_token = jnp.sum(expert_hits, axis=1)
    earlier = jnp.cumsum(per_token, axis=0) - per_token
    route_rank = jnp.sum(expert_hits * earlier[:, None, :], axis=2)
    is_kept = route_rank < capacity
    slot_index = target * capacity + jnp.minimum(route_rank, capacity - 1)
    return (slot_index, is_kept)


def slot_sources(slot_index, is_kept, slot_count):
    token_ids = jnp.broadcast_to(
        jnp.arange(slot_index.shape[0], dtype=jnp.int32)[:, None], slot_index.shape
    )
    placed = jnp.where(is_kept, slot_index, slot_count).reshape(-1)
    source = jnp.zeros((slot_count,), jnp.int32).at[placed].set(token_ids.reshape(-1), mode="drop")
    slot_used = jnp.zeros((slot_count,), jnp.bool_).at[placed].set(True, mode="drop")
    return (source, slot_used)


def per_device(
    mix_input,
    pool_weight,
    pool_scale,
    out_weight,
    moe_input,
    moe_gain,
    group_router,
    inner_router,
    group_pick,
    inner_pick,
    gate_weight,
    up_weight,
    down_weight,
):
    row_count = mix_input.shape[0]
    reach_back = WINDOW_MAX - 1
    before = passed_along(mix_input[row_count - reach_back :], ("ep", "tp"), 1)
    extended = jnp.concatenate([before, mix_input], axis=0).astype(jnp.float32)
    first_position = lax.axis_index(("ep", "tp")) * row_count
    trailing = (
        trailing_means(extended, row_count, reach_back, first_position) - extended[reach_back:]
    )
    pooled = trailing.astype(jnp.bfloat16)
    groups, group_dim = (pool_weight.shape[0], pool_weight.shape[1])
    grouped = jnp.einsum(
        "tgc,gcd->tgd",
        pooled.reshape(row_count, groups, group_dim),
        pool_weight,
        preferred_element_type=jnp.float32,
    )
    grouped = (grouped.reshape(row_count, groups * group_dim) * pool_scale[None, :]).astype(
        jnp.bfloat16
    )
    mix_out = jnp.dot(grouped, out_weight, preferred_element_type=jnp.float32).astype(jnp.bfloat16)
    tokens, feature_width = moe_input.shape
    token_values = moe_input.astype(jnp.float32)
    norm_scale = lax.rsqrt(
        jnp.maximum(jnp.mean(token_values * token_values, axis=1, keepdims=True), NORM_FLOOR)
    )
    normed = (token_values * norm_scale * moe_gain[None, :]).astype(jnp.bfloat16)
    group_logits = jnp.dot(normed, group_router, preferred_element_type=jnp.float32)
    inner_logits = jnp.dot(normed, inner_router, preferred_element_type=jnp.float32)
    group_count = group_router.shape[1]
    expert_count = inner_router.shape[1]
    target, route_weight = route_terms(
        group_logits, inner_logits, group_pick, inner_pick, expert_count // group_count
    )
    capacity = 2 * inner_pick.shape[1] * tokens // expert_count
    slot_index, is_kept = slot_terms(target, expert_count, capacity)
    source, slot_used = slot_sources(slot_index, is_kept, expert_count * capacity)
    gate_local = gate_weight[0]
    up_local = up_weight[0]
    outgoing = jnp.where(slot_used[:, None], normed[source], jnp.zeros((), jnp.bfloat16))
    arrived = lax.all_to_all(outgoing, "ep", split_axis=0, concat_axis=0, tiled=True)
    gate_sum = jnp.dot(arrived, gate_local, preferred_element_type=jnp.float32)
    up_sum = jnp.dot(arrived, up_local, preferred_element_type=jnp.float32)
    hidden = (jax.nn.silu(gate_sum) * up_sum).astype(jnp.bfloat16)
    down_local = down_weight[0]
    expert_result = lax.psum_scatter(
        lax.dot_general(
            down_local, hidden, (((0,), (1,)), ((), ())), preferred_element_type=jnp.float32
        ).astype(jnp.bfloat16),
        "tp",
        scatter_dimension=0,
        tiled=True,
    )
    returned = lax.all_to_all(expert_result, "ep", split_axis=1, concat_axis=1, tiled=True)
    route_scale = jnp.where(is_kept, route_weight, 0.0).astype(jnp.bfloat16)
    route_scale = lax.optimization_barrier(route_scale).astype(jnp.float32)
    picked = jnp.take(returned, slot_index, axis=1).astype(jnp.float32)
    combined = jnp.sum(picked * route_scale[None, :, :], axis=2)
    moe_out = combined.T.astype(jnp.bfloat16)
    return (mix_out, moe_out)


def flipped(index, mask, count):
    total = 0
    bit = 1
    while bit < count:
        own = (index // bit) % 2
        total = total + bit * ((1 - own) if mask & bit else own)
        bit *= 2
    return total


def fused_kernel(
    n,
    capacity,
    per_group,
    mix_ref,
    pool_w_ref,
    pool_s_ref,
    out_w_hbm,
    moe_ref,
    gain_ref,
    group_rt_ref,
    inner_rt_ref,
    gp_ref,
    ip_ref,
    gate_hbm,
    up_hbm,
    down_hbm,
    mix_out_ref,
    moe_out_ref,
    out_w,
    gate_w,
    up_w,
    down_w,
    halo,
    pooled_v,
    grouped_v,
    normed_v,
    outgoing,
    arrived,
    part_own,
    part_send,
    part_recv,
    result,
    returned,
    combine_w,
    slot_info,
    raw_info,
    raw_rows,
    relayed,
    load_sem,
    halo_sem,
    sent_sem,
    recv_sem,
    swap_recv,
    part_recv_sem,
    ret_recv,
    raw_sem,
):
    ep, tp = lax.axis_index("ep"), lax.axis_index("tp")
    other = 1 - tp
    total_devices = 2 * n
    linear = ep * 2 + tp
    following = lax.rem(linear + 1, total_devices)
    preceding = lax.rem(linear + total_devices - 1, total_devices)
    tokens, width = moe_ref.shape
    half = width // 2
    rows = mix_ref.shape[0]
    slots = n * capacity
    near = n // 2
    low, high = (ep // CHUNK) % 2, (ep // near) % 2
    inner = low + high - 2 * low * high

    barrier = pltpu.get_barrier_semaphore()
    greeted = [(flipped(ep, j, n), tp) for j in range(1, n)]
    greeted += [(ep, other), (following // 2, following % 2), (preceding // 2, preceding % 2)]
    for device in greeted:
        pl.semaphore_signal(barrier, inc=1, device_id=device, device_id_type=MESH)

    loads = [
        pltpu.make_async_copy(gate_hbm.at[0], gate_w, load_sem.at[0]),
        pltpu.make_async_copy(up_hbm.at[0], up_w, load_sem.at[1]),
        pltpu.make_async_copy(out_w_hbm, out_w, load_sem.at[2]),
        pltpu.make_async_copy(down_hbm.at[0, :, pl.ds(0, half)], down_w.at[0], load_sem.at[3]),
        pltpu.make_async_copy(down_hbm.at[0, :, pl.ds(half, half)], down_w.at[1], load_sem.at[4]),
    ]
    for index in (0, 1, 3, 4, 2):
        loads[index].start()

    values = moe_ref[...].astype(jnp.float32)
    scale = lax.rsqrt(
        jnp.maximum(jnp.sum(values * values, axis=1, keepdims=True) * (1.0 / width), NORM_FLOOR)
    )
    normed = (values * scale * gain_ref[...]).astype(jnp.bfloat16)
    for part in range(2):
        normed_v[part] = normed[:, part * half : (part + 1) * half]

    group_pick = gp_ref[...]
    expert_count = inner_rt_ref.shape[0]
    targets = [group_pick * per_group + ip_ref[k : k + 1, :] for k in range(2)]
    expert_ids = lax.broadcasted_iota(jnp.int32, (expert_count, tokens), 0)
    hits = [expert_ids == target for target in targets]
    both = (hits[0].astype(jnp.float32) + hits[1].astype(jnp.float32)).astype(jnp.bfloat16)
    earlier_mask = (
        lax.broadcasted_iota(jnp.int32, (tokens, tokens), 0)
        < lax.broadcasted_iota(jnp.int32, (tokens, tokens), 1)
    ).astype(jnp.float32).astype(jnp.bfloat16)
    earlier = jnp.dot(both, earlier_mask, preferred_element_type=jnp.float32)
    slot_of = []
    for k in range(2):
        rank = jnp.sum(jnp.where(hits[k], earlier, 0.0), axis=0, keepdims=True).astype(jnp.int32)
        slot_of.append(jnp.where(rank < capacity, targets[k] * capacity + rank, -1))
    slot_ids = lax.broadcasted_iota(jnp.int32, (slots, tokens), 0)
    chosen = [slot_ids == slot for slot in slot_of]
    pick = jnp.where(chosen[0] | chosen[1], 1.0, 0.0).astype(jnp.bfloat16)
    for part in range(2):
        outgoing[part] = jnp.dot(
            pick, normed_v[part], preferred_element_type=jnp.float32
        ).astype(jnp.bfloat16)
    for k in range(2):
        slot_info[k : k + 1, :] = slot_of[k]

    pl.semaphore_wait(barrier, len(greeted))

    own_rows = pl.ds(pl.multiple_of(ep * capacity, capacity), capacity)
    halo_copy = pltpu.make_async_remote_copy(
        src_ref=mix_ref.at[pl.ds(rows - LEAD, LEAD)],
        dst_ref=halo,
        send_sem=halo_sem.at[0],
        recv_sem=halo_sem.at[1],
        device_id=(following // 2, following % 2),
        device_id_type=MESH,
    )
    halo_copy.start()

    relay_lanes = [slice(first, first + half // 2) for first in range(0, half, half // 2)]

    def rows_of(index):
        return pl.ds(pl.multiple_of(index * capacity, capacity), capacity)

    def partner(k):
        there = flipped(ep, k, n)
        if k < near:
            return k, there
        shift = CHUNK if k < near + CHUNK else -CHUNK
        return k + inner * shift, there + inner * (CHUNK - 2 * CHUNK * ((there // CHUNK) % 2))

    def pair_rows(k):
        start = partner(k)[1] // 2 * (2 * capacity)
        return pl.ds(pl.multiple_of(start, 2 * capacity), 2 * capacity)

    def remote(src, dst, sent, received, device):
        return pltpu.make_async_remote_copy(
            src_ref=src,
            dst_ref=dst,
            send_sem=sent,
            recv_sem=received,
            device_id=device,
            device_id_type=MESH,
        )

    def landed(ref, semaphore):
        remote(ref, ref, sent_sem.at[0], semaphore, (ep, other)).wait_recv()

    def all_sent(ref, semaphore):
        remote(ref, ref, semaphore, ret_recv.at[0], (ep, other)).wait_send()

    def dispatch(k):
        j, there = partner(k)
        if k < near:
            src, dst = outgoing.at[:, rows_of(there)], arrived.at[:, own_rows]
            sent, received = sent_sem.at[0], recv_sem.at[k // 2]
        else:
            src, dst = outgoing.at[tp, rows_of(there)], arrived.at[tp, own_rows]
            sent, received = sent_sem.at[1], recv_sem.at[near // 2 + j - near]
        return remote(src, dst, sent, received, (there, tp))

    def swap(k):
        block = arrived.at[tp, rows_of(partner(k)[1])]
        received = swap_recv.at[(k - near) // 2]
        return remote(block, block, sent_sem.at[2], received, (ep, other))

    def partial_copy(k):
        block = rows_of(partner(k)[1])
        received = part_recv_sem.at[k // 2 if k < near + CHUNK else k - near // 2 - CHUNK // 2]
        return remote(
            part_send.at[block], part_recv.at[block], sent_sem.at[3], received, (ep, other)
        )

    def give_back(k):
        there = partner(k)[1]
        return remote(
            result.at[rows_of(there)],
            returned.at[own_rows],
            sent_sem.at[4],
            ret_recv.at[0],
            (there, tp),
        )

    raw_copies = [
        remote(src, dst, raw_sem.at[min(index, 1)], raw_sem.at[2 + index], (flipped(ep, near, n), tp))
        for index, (src, dst) in enumerate(
            [(slot_info, raw_info)]
            + [(normed_v.at[tp, :, lanes], raw_rows.at[:, lanes]) for lanes in relay_lanes]
        )
    ]

    def relay_copy(m, lanes):
        there = flipped(ep, m, n)
        return remote(
            relayed.at[rows_of(there % near), lanes],
            arrived.at[tp, rows_of(flipped(ep, near, n)), lanes],
            sent_sem.at[5],
            recv_sem.at[near // 2 + m],
            (there, tp),
        )

    relay_order = list(range(CHUNK, near)) + list(range(1, CHUNK))

    def relay():
        raw_copies[0].wait_recv()
        first_slot = (ep // near) * (near * capacity)
        half_ids = lax.broadcasted_iota(jnp.int32, (near * capacity, tokens), 0) + first_slot
        half_pick = jnp.where(
            (half_ids == raw_info[0:1, :]) | (half_ids == raw_info[1:2, :]), 1.0, 0.0
        ).astype(jnp.bfloat16)
        for index, lanes in enumerate(relay_lanes):
            raw_copies[1 + index].wait_recv()
            relayed[:, lanes] = jnp.dot(
                half_pick, raw_rows[:, lanes], preferred_element_type=jnp.float32
            ).astype(jnp.bfloat16)
            for m in relay_order:
                relay_copy(m, lanes).start()
            arrived[tp, rows_of(flipped(ep, near, n)), lanes] = relayed[rows_of(ep % near), lanes]

    def sends_outer():
        for copy in raw_copies:
            copy.start()

    def sends_inner():
        for k in range(near, n):
            dispatch(k).start()

    def sent_outer():
        raw_copies[0].wait_send()
        all_sent(normed_v.at[tp], raw_sem.at[1])

    def sent_inner():
        all_sent(outgoing.at[0, pl.ds(0, near * capacity)], sent_sem.at[1])
        all_sent(relayed.at[pl.ds(0, (near - 1) * capacity)], sent_sem.at[5])

    for k in range(1, near):
        dispatch(k).start()
    pl.when(inner == 0)(sends_outer)
    pl.when(inner == 1)(sends_inner)
    arrived[:, own_rows] = outgoing[:, own_rows]

    def contract(left, right):
        return lax.dot_general(
            left, right, (((1,), (1,)), ((), ())), preferred_element_type=jnp.float32
        )

    def logits_of(router):
        return contract(router[:, :half], normed_v[0]) + contract(router[:, half:], normed_v[1])

    group_logits = logits_of(group_rt_ref)
    inner_logits = logits_of(inner_rt_ref)
    group_ids = lax.broadcasted_iota(jnp.int32, group_logits.shape, 0)
    own_logit = jnp.sum(
        jnp.where(group_ids == group_pick, group_logits, 0.0), axis=0, keepdims=True
    )
    share = 1.0 / jnp.sum(jnp.exp(group_logits - own_logit), axis=0, keepdims=True)
    picked = [
        jnp.sum(jnp.where(hit, inner_logits, 0.0), axis=0, keepdims=True) for hit in hits
    ]
    first = jax.nn.sigmoid(picked[0] - picked[1])
    weights = [
        (share * value).astype(jnp.bfloat16).astype(jnp.float32) for value in (first, 1.0 - first)
    ]
    spread = jnp.where(chosen[0], weights[0], 0.0) + jnp.where(chosen[1], weights[1], 0.0)
    combine_w[...] = spread.T.astype(jnp.bfloat16)

    def mixer():
        halo_copy.wait()
        group_width = mix_ref.shape[1] // 4
        position = linear * rows + lax.broadcasted_iota(jnp.int32, (rows, 1), 0)
        is_first = linear == 0
        for index in range(4):
            window = 2 ** (index + 1)
            lanes = slice(index * group_width, (index + 1) * group_width)
            lead = jnp.where(is_first, 0.0, halo[:, lanes].astype(jnp.float32))
            body = mix_ref[:, lanes].astype(jnp.float32)
            sums = jnp.concatenate([lead, body], axis=0)
            shift = 1
            while shift < window:
                sums = sums + pltpu.roll(sums, shift, 0)
                shift *= 2
            inverse = 1.0 / jnp.minimum(position + 1, window).astype(jnp.float32)
            pooled_v[:, lanes] = (sums[LEAD:] * inverse - body).astype(jnp.bfloat16)
        group_dim = pool_w_ref.shape[1]
        for g in range(pool_w_ref.shape[0]):
            lanes = slice(g * group_dim, (g + 1) * group_dim)
            product = jnp.dot(pooled_v[:, lanes], pool_w_ref[g], preferred_element_type=jnp.float32)
            grouped_v[:, lanes] = (product * pool_s_ref[:, lanes]).astype(jnp.bfloat16)
        loads[2].wait()
        tile = 512

        @pl.loop(0, mix_out_ref.shape[1] // tile)
        def _(step):
            lanes = pl.ds(pl.multiple_of(step * tile, tile), tile)
            mix_out_ref[:, lanes] = jnp.dot(
                grouped_v[...], out_w[:, lanes], preferred_element_type=jnp.float32
            ).astype(jnp.bfloat16)

    groups = [list(range(first, first + CHUNK)) for first in range(0, n, CHUNK)]

    def expert(group):
        size = len(group)
        start = partner(group[0])[1] // size * (size * capacity)
        span = pl.ds(pl.multiple_of(start, size * capacity), size * capacity)
        sums = []
        for weight in (gate_w, up_w):
            sums.append(
                jnp.dot(arrived[0, span], weight[:half], preferred_element_type=jnp.float32)
                + jnp.dot(arrived[1, span], weight[half:], preferred_element_type=jnp.float32)
            )
        hidden = (sums[0] / (1.0 + jnp.exp(-sums[0])) * sums[1]).astype(jnp.bfloat16)

        def part(index):
            return jnp.dot(
                hidden, down_w[index], preferred_element_type=jnp.float32
            ).astype(jnp.bfloat16)

        part_send[span] = part(other)
        for k in group:
            partial_copy(k).start()
        part_own[span] = part(tp)

    def add_up(block):
        result[block] = (
            part_own[block].astype(jnp.float32) + part_recv[block].astype(jnp.float32)
        ).astype(jnp.bfloat16)

    def finish_one(k):
        partial_copy(k).wait_recv()
        add_up(rows_of(partner(k)[1]))
        give_back(k).start()

    def finish(pair):
        block = pair_rows(pair[0])
        landed(part_recv.at[block], part_recv_sem.at[pair[0] // 2])
        add_up(block)
        for k in pair:
            if k:
                give_back(k).start()
        if pair[0] == 0:
            returned[own_rows] = result[own_rows]

    def pass_on(k):
        if k == near + CHUNK:
            pl.when(inner == 0)(dispatch(k).wait_recv)
        else:
            dispatch(k).wait_recv()
        swap(k).start()

    def straight(pair):
        if pair[0] == 0:
            dispatch(1).wait_recv()
        else:
            landed(arrived.at[:, pair_rows(pair[0])], recv_sem.at[pair[0] // 2])
        expert(pair)

    def swapped(pair):
        landed(arrived.at[other, pair_rows(pair[0])], swap_recv.at[(pair[0] - near) // 2])
        expert(pair)

    early, late, beside, beyond, far, farther, last, latest = [
        [first, first + 1] for first in range(0, n, 2)
    ]

    def late_plane():
        straight(late)

    def late_back():
        finish(late)

    for index in (0, 1, 3, 4):
        loads[index].wait()
    straight(early)
    mixer()
    pl.when(inner == 0)(late_plane)
    for k in far + farther:
        pass_on(k)
    finish(early)
    pl.when(inner == 0)(late_back)
    swapped(far)
    swapped(farther)
    straight(beside)
    straight(beyond)
    finish(far)
    pl.when(inner == 1)(relay)
    finish(farther)
    for k in last + latest:
        pass_on(k)
    finish(beside)
    finish(beyond)
    swapped(last)
    swapped(latest)
    pl.when(inner == 1)(late_plane)
    for k in last + latest:
        finish_one(k)
    pl.when(inner == 1)(late_back)
    landed(returned.at[pl.ds(0, (n - 1) * capacity)], ret_recv.at[0])
    moe_out_ref[...] = jnp.dot(
        combine_w[...], returned[...], preferred_element_type=jnp.float32
    ).astype(jnp.bfloat16)
    pl.when(inner == 0)(sent_outer)
    pl.when(inner == 1)(sent_inner)
    all_sent(outgoing.at[:, pl.ds(0, (near - 1) * capacity)], sent_sem.at[0])
    all_sent(arrived.at[0, pl.ds(0, near * capacity)], sent_sem.at[2])
    all_sent(part_send, sent_sem.at[3])
    all_sent(result.at[pl.ds(0, (n - 1) * capacity)], sent_sem.at[4])


def fused(
    mix_input,
    pool_weight,
    pool_scale,
    out_weight,
    moe_input,
    moe_gain,
    group_router,
    inner_router,
    group_pick,
    inner_pick,
    gate_weight,
    up_weight,
    down_weight,
):
    n = lax.axis_size("ep")
    tokens, width = moe_input.shape
    rows, channels = mix_input.shape
    expert_count = inner_router.shape[1]
    capacity = 2 * inner_pick.shape[1] * tokens // expert_count
    half = width // 2
    slots = n * capacity
    hidden = gate_weight.shape[2]
    bf16 = jnp.bfloat16
    vmem = pl.BlockSpec(memory_space=pltpu.VMEM)
    hbm = pl.BlockSpec(memory_space=pl.ANY)
    dma = pltpu.SemaphoreType.DMA
    return pl.pallas_call(
        functools.partial(
            fused_kernel, n, capacity, expert_count // group_router.shape[1]
        ),
        out_shape=(
            pltpu.VMEM((rows, out_weight.shape[1]), bf16),
            pltpu.VMEM((tokens, half), bf16),
        ),
        in_specs=[vmem, vmem, vmem, hbm] + [vmem] * 6 + [hbm] * 3,
        out_specs=(vmem, vmem),
        scratch_shapes=[
            pltpu.VMEM(out_weight.shape, bf16),
            pltpu.VMEM((width, hidden), bf16),
            pltpu.VMEM((width, hidden), bf16),
            pltpu.VMEM((2, hidden, half), bf16),
            pltpu.VMEM((LEAD, channels), bf16),
            pltpu.VMEM((rows, channels), bf16),
            pltpu.VMEM((rows, channels), bf16),
            pltpu.VMEM((2, tokens, half), bf16),
            pltpu.VMEM((2, slots, half), bf16),
            pltpu.VMEM((2, slots, half), bf16),
            pltpu.VMEM((slots, half), bf16),
            pltpu.VMEM((slots, half), bf16),
            pltpu.VMEM((slots, half), bf16),
            pltpu.VMEM((slots, half), bf16),
            pltpu.VMEM((slots, half), bf16),
            pltpu.VMEM((tokens, slots), bf16),
            pltpu.VMEM((2, tokens), jnp.int32),
            pltpu.VMEM((2, tokens), jnp.int32),
            pltpu.VMEM((tokens, half), bf16),
            pltpu.VMEM((slots // 2, half), bf16),
            dma((5,)),
            dma((2,)),
            dma((6,)),
            dma((n // 2 + n // 4,)),
            dma((n // 4,)),
            dma((n // 2 + n // 8,)),
            dma((1,)),
            dma((5,)),
        ],
        compiler_params=pltpu.CompilerParams(
            collective_id=0, has_side_effects=True, vmem_limit_bytes=60 * 1024 * 1024
        ),
    )(
        mix_input,
        pool_weight,
        pool_scale[None, :],
        out_weight,
        moe_input,
        moe_gain[None, :],
        group_router.T,
        inner_router.T,
        group_pick[None, :],
        inner_pick.T,
        gate_weight,
        up_weight,
        down_weight,
    )


def step(*arrays):
    mix_input, moe_input, inner_router, inner_pick = arrays[0], arrays[4], arrays[7], arrays[9]
    n, n_tp = lax.axis_size("ep"), lax.axis_size("tp")
    capacity = 2 * inner_pick.shape[1] * moe_input.shape[0] // inner_router.shape[1]
    fits = (
        n_tp == 2
        and inner_pick.shape[1] == 2
        and n == 4 * CHUNK
        and inner_router.shape[1] == n
        and capacity % 16 == 0
        and mix_input.shape[0] >= LEAD
    )
    return fused(*arrays) if fits else per_device(*arrays)


def solution(mesh):
    in_specs = (
        P(("ep", "tp"), None),
        P(),
        P(),
        P(),
        P("ep", None),
        P(),
        P(),
        P(),
        P("ep"),
        P("ep", None),
        P("ep", None, "tp"),
        P("ep", None, "tp"),
        P("ep", "tp", None),
    )
    out_specs = (P(("ep", "tp"), None), P("ep", "tp"))
    return jax.shard_map(
        step, mesh=mesh, in_specs=in_specs, out_specs=out_specs, check_vma=False
    )
```

```python
import functools

import jax
import jax.numpy as jnp
from jax import lax
from jax.experimental import pallas as pl
from jax.experimental.pallas import tpu as pltpu
from jax.sharding import PartitionSpec as P

MESH = pl.DeviceIdType.MESH
CHUNK = 4
LEAD = 16

WINDOW_MAX = 16


NORM_FLOOR = 0.25


def passed_along(value, axis, steps):
    count = lax.axis_size(axis)
    first, last = (max(0, -steps), min(count, count - steps))
    return lax.ppermute(value, axis, [(source, source + steps) for source in range(first, last)])


def trailing_means(extended, row_count, lead_rows, first_position):
    group_width = extended.shape[1] // 4
    position = first_position + jnp.arange(row_count, dtype=jnp.int32)
    pieces = []
    for scale_index in range(4):
        window = 2 ** (scale_index + 1)
        channel_block = extended[:, scale_index * group_width : (scale_index + 1) * group_width]
        window_sum = channel_block[lead_rows : lead_rows + row_count]
        for back_step in range(1, window):
            window_sum = (
                window_sum
                + channel_block[lead_rows - back_step : lead_rows - back_step + row_count]
            )
        divisor = jnp.minimum(position + 1, window).astype(jnp.float32)
        pieces.append(window_sum / divisor[:, None])
    return jnp.concatenate(pieces, axis=1)


def route_terms(group_logits, inner_logits, group_pick, inner_pick, per_group):
    group_ids = jnp.arange(group_logits.shape[1], dtype=jnp.int32)
    chosen = jnp.sum(
        jnp.where(group_pick[:, None] == group_ids[None, :], group_logits, 0.0), axis=1
    )
    group_share = 1.0 / jnp.sum(jnp.exp(group_logits - chosen[:, None]), axis=1)
    target = group_pick[:, None] * per_group + inner_pick
    expert_ids = jnp.arange(inner_logits.shape[1], dtype=jnp.int32)
    picked = jnp.sum(
        jnp.where(target[:, :, None] == expert_ids[None, None, :], inner_logits[:, None, :], 0.0),
        axis=2,
    )
    first_share = jax.nn.sigmoid(picked[:, 0] - picked[:, 1])
    route_weight = group_share[:, None] * jnp.stack([first_share, 1.0 - first_share], axis=1)
    return (target, route_weight)


def slot_terms(target, expert_count, capacity):
    expert_ids = jnp.arange(expert_count, dtype=jnp.int32)
    expert_hits = (target[:, :, None] == expert_ids[None, None, :]).astype(jnp.int32)
    per_token = jnp.sum(expert_hits, axis=1)
    earlier = jnp.cumsum(per_token, axis=0) - per_token
    route_rank = jnp.sum(expert_hits * earlier[:, None, :], axis=2)
    is_kept = route_rank < capacity
    slot_index = target * capacity + jnp.minimum(route_rank, capacity - 1)
    return (slot_index, is_kept)


def slot_sources(slot_index, is_kept, slot_count):
    token_ids = jnp.broadcast_to(
        jnp.arange(slot_index.shape[0], dtype=jnp.int32)[:, None], slot_index.shape
    )
    placed = jnp.where(is_kept, slot_index, slot_count).reshape(-1)
    source = jnp.zeros((slot_count,), jnp.int32).at[placed].set(token_ids.reshape(-1), mode="drop")
    slot_used = jnp.zeros((slot_count,), jnp.bool_).at[placed].set(True, mode="drop")
    return (source, slot_used)


def per_device(
    mix_input,
    pool_weight,
    pool_scale,
    out_weight,
    moe_input,
    moe_gain,
    group_router,
    inner_router,
    group_pick,
    inner_pick,
    gate_weight,
    up_weight,
    down_weight,
):
    row_count = mix_input.shape[0]
    reach_back = WINDOW_MAX - 1
    before = passed_along(mix_input[row_count - reach_back :], ("ep", "tp"), 1)
    extended = jnp.concatenate([before, mix_input], axis=0).astype(jnp.float32)
    first_position = lax.axis_index(("ep", "tp")) * row_count
    trailing = (
        trailing_means(extended, row_count, reach_back, first_position) - extended[reach_back:]
    )
    pooled = trailing.astype(jnp.bfloat16)
    groups, group_dim = (pool_weight.shape[0], pool_weight.shape[1])
    grouped = jnp.einsum(
        "tgc,gcd->tgd",
        pooled.reshape(row_count, groups, group_dim),
        pool_weight,
        preferred_element_type=jnp.float32,
    )
    grouped = (grouped.reshape(row_count, groups * group_dim) * pool_scale[None, :]).astype(
        jnp.bfloat16
    )
    mix_out = jnp.dot(grouped, out_weight, preferred_element_type=jnp.float32).astype(jnp.bfloat16)
    tokens, feature_width = moe_input.shape
    token_values = moe_input.astype(jnp.float32)
    norm_scale = lax.rsqrt(
        jnp.maximum(jnp.mean(token_values * token_values, axis=1, keepdims=True), NORM_FLOOR)
    )
    normed = (token_values * norm_scale * moe_gain[None, :]).astype(jnp.bfloat16)
    group_logits = jnp.dot(normed, group_router, preferred_element_type=jnp.float32)
    inner_logits = jnp.dot(normed, inner_router, preferred_element_type=jnp.float32)
    group_count = group_router.shape[1]
    expert_count = inner_router.shape[1]
    target, route_weight = route_terms(
        group_logits, inner_logits, group_pick, inner_pick, expert_count // group_count
    )
    capacity = 2 * inner_pick.shape[1] * tokens // expert_count
    slot_index, is_kept = slot_terms(target, expert_count, capacity)
    source, slot_used = slot_sources(slot_index, is_kept, expert_count * capacity)
    gate_local = gate_weight[0]
    up_local = up_weight[0]
    outgoing = jnp.where(slot_used[:, None], normed[source], jnp.zeros((), jnp.bfloat16))
    arrived = lax.all_to_all(outgoing, "ep", split_axis=0, concat_axis=0, tiled=True)
    gate_sum = jnp.dot(arrived, gate_local, preferred_element_type=jnp.float32)
    up_sum = jnp.dot(arrived, up_local, preferred_element_type=jnp.float32)
    hidden = (jax.nn.silu(gate_sum) * up_sum).astype(jnp.bfloat16)
    down_local = down_weight[0]
    expert_result = lax.psum_scatter(
        lax.dot_general(
            down_local, hidden, (((0,), (1,)), ((), ())), preferred_element_type=jnp.float32
        ).astype(jnp.bfloat16),
        "tp",
        scatter_dimension=0,
        tiled=True,
    )
    returned = lax.all_to_all(expert_result, "ep", split_axis=1, concat_axis=1, tiled=True)
    route_scale = jnp.where(is_kept, route_weight, 0.0).astype(jnp.bfloat16)
    route_scale = lax.optimization_barrier(route_scale).astype(jnp.float32)
    picked = jnp.take(returned, slot_index, axis=1).astype(jnp.float32)
    combined = jnp.sum(picked * route_scale[None, :, :], axis=2)
    moe_out = combined.T.astype(jnp.bfloat16)
    return (mix_out, moe_out)


def flipped(index, mask, count):
    total = 0
    bit = 1
    while bit < count:
        own = (index // bit) % 2
        total = total + bit * ((1 - own) if mask & bit else own)
        bit *= 2
    return total


def fused_kernel(
    n,
    capacity,
    per_group,
    mix_ref,
    pool_w_ref,
    pool_s_ref,
    out_w_hbm,
    moe_ref,
    gain_ref,
    group_rt_ref,
    inner_rt_ref,
    gp_ref,
    ip_ref,
    gate_hbm,
    up_hbm,
    down_hbm,
    mix_out_ref,
    moe_out_ref,
    out_w,
    gate_w,
    up_w,
    down_w,
    halo,
    pooled_v,
    grouped_v,
    normed_v,
    outgoing,
    arrived,
    part_own,
    part_send,
    part_recv,
    result,
    returned,
    combine_w,
    slot_info,
    raw_info,
    raw_rows,
    relayed,
    load_sem,
    halo_sem,
    sent_sem,
    recv_sem,
    swap_recv,
    part_recv_sem,
    ret_recv,
    raw_sem,
):
    ep, tp = lax.axis_index("ep"), lax.axis_index("tp")
    other = 1 - tp
    total_devices = 2 * n
    linear = ep * 2 + tp
    following = lax.rem(linear + 1, total_devices)
    preceding = lax.rem(linear + total_devices - 1, total_devices)
    tokens, width = moe_ref.shape
    half = width // 2
    rows = mix_ref.shape[0]
    slots = n * capacity
    near = n // 2
    low, high = (ep // CHUNK) % 2, (ep // near) % 2
    inner = low + high - 2 * low * high

    barrier = pltpu.get_barrier_semaphore()
    greeted = [(flipped(ep, j, n), tp) for j in range(1, n)]
    greeted += [(ep, other), (following // 2, following % 2), (preceding // 2, preceding % 2)]
    for device in greeted:
        pl.semaphore_signal(barrier, inc=1, device_id=device, device_id_type=MESH)

    loads = [
        pltpu.make_async_copy(gate_hbm.at[0], gate_w, load_sem.at[0]),
        pltpu.make_async_copy(up_hbm.at[0], up_w, load_sem.at[1]),
        pltpu.make_async_copy(out_w_hbm, out_w, load_sem.at[2]),
        pltpu.make_async_copy(down_hbm.at[0, :, pl.ds(0, half)], down_w.at[0], load_sem.at[3]),
        pltpu.make_async_copy(down_hbm.at[0, :, pl.ds(half, half)], down_w.at[1], load_sem.at[4]),
    ]
    for index in (0, 1, 3, 4, 2):
        loads[index].start()

    values = moe_ref[...].astype(jnp.float32)
    scale = lax.rsqrt(
        jnp.maximum(jnp.sum(values * values, axis=1, keepdims=True) * (1.0 / width), NORM_FLOOR)
    )
    normed = (values * scale * gain_ref[...]).astype(jnp.bfloat16)
    for part in range(2):
        normed_v[part] = normed[:, part * half : (part + 1) * half]

    group_pick = gp_ref[...]
    expert_count = inner_rt_ref.shape[0]
    targets = [group_pick * per_group + ip_ref[k : k + 1, :] for k in range(2)]
    expert_ids = lax.broadcasted_iota(jnp.int32, (expert_count, tokens), 0)
    hits = [expert_ids == target for target in targets]
    both = (hits[0].astype(jnp.float32) + hits[1].astype(jnp.float32)).astype(jnp.bfloat16)
    earlier_mask = (
        lax.broadcasted_iota(jnp.int32, (tokens, tokens), 0)
        < lax.broadcasted_iota(jnp.int32, (tokens, tokens), 1)
    ).astype(jnp.float32).astype(jnp.bfloat16)
    earlier = jnp.dot(both, earlier_mask, preferred_element_type=jnp.float32)
    slot_of = []
    for k in range(2):
        rank = jnp.sum(jnp.where(hits[k], earlier, 0.0), axis=0, keepdims=True).astype(jnp.int32)
        slot_of.append(jnp.where(rank < capacity, targets[k] * capacity + rank, -1))
    slot_ids = lax.broadcasted_iota(jnp.int32, (slots, tokens), 0)
    chosen = [slot_ids == slot for slot in slot_of]
    pick = jnp.where(chosen[0] | chosen[1], 1.0, 0.0).astype(jnp.bfloat16)
    for part in range(2):
        outgoing[part] = jnp.dot(
            pick, normed_v[part], preferred_element_type=jnp.float32
        ).astype(jnp.bfloat16)
    for k in range(2):
        slot_info[k : k + 1, :] = slot_of[k]

    pl.semaphore_wait(barrier, len(greeted))

    own_rows = pl.ds(pl.multiple_of(ep * capacity, capacity), capacity)
    halo_copy = pltpu.make_async_remote_copy(
        src_ref=mix_ref.at[pl.ds(rows - LEAD, LEAD)],
        dst_ref=halo,
        send_sem=halo_sem.at[0],
        recv_sem=halo_sem.at[1],
        device_id=(following // 2, following % 2),
        device_id_type=MESH,
    )
    halo_copy.start()

    relay_lanes = [slice(first, first + half // 2) for first in range(0, half, half // 2)]

    def rows_of(index):
        return pl.ds(pl.multiple_of(index * capacity, capacity), capacity)

    def partner(k):
        there = flipped(ep, k, n)
        if k < near:
            return k, there
        shift = CHUNK if k < near + CHUNK else -CHUNK
        return k + inner * shift, there + inner * (CHUNK - 2 * CHUNK * ((there // CHUNK) % 2))

    def pair_rows(k):
        start = partner(k)[1] // 2 * (2 * capacity)
        return pl.ds(pl.multiple_of(start, 2 * capacity), 2 * capacity)

    def remote(src, dst, sent, received, device):
        return pltpu.make_async_remote_copy(
            src_ref=src,
            dst_ref=dst,
            send_sem=sent,
            recv_sem=received,
            device_id=device,
            device_id_type=MESH,
        )

    def landed(ref, semaphore):
        remote(ref, ref, sent_sem.at[0], semaphore, (ep, other)).wait_recv()

    def all_sent(ref, semaphore):
        remote(ref, ref, semaphore, ret_recv.at[0], (ep, other)).wait_send()

    def dispatch(k):
        j, there = partner(k)
        if k < near:
            src, dst = outgoing.at[:, rows_of(there)], arrived.at[:, own_rows]
            sent, received = sent_sem.at[0], recv_sem.at[near // 2 + near if k == 2 else k // 2]
        else:
            src, dst = outgoing.at[tp, rows_of(there)], arrived.at[tp, own_rows]
            sent, received = sent_sem.at[1], recv_sem.at[near // 2 + j - near]
        return remote(src, dst, sent, received, (there, tp))

    def swap(k):
        block = arrived.at[tp, rows_of(partner(k)[1])]
        received = swap_recv.at[(k - near) // 2]
        return remote(block, block, sent_sem.at[2], received, (ep, other))

    def partial_copy(k):
        block = rows_of(partner(k)[1])
        received = part_recv_sem.at[k]
        return remote(
            part_send.at[block], part_recv.at[block], sent_sem.at[3], received, (ep, other)
        )

    def give_back(k):
        there = partner(k)[1]
        return remote(
            result.at[rows_of(there)],
            returned.at[own_rows],
            sent_sem.at[4],
            ret_recv.at[0],
            (there, tp),
        )

    raw_copies = [
        remote(src, dst, raw_sem.at[min(index, 1)], raw_sem.at[2 + index], (flipped(ep, near, n), tp))
        for index, (src, dst) in enumerate(
            [(slot_info, raw_info)]
            + [(normed_v.at[tp, :, lanes], raw_rows.at[:, lanes]) for lanes in relay_lanes]
        )
    ]

    def relay_copy(m, lanes):
        there = flipped(ep, m, n)
        return remote(
            relayed.at[rows_of(there % near), lanes],
            arrived.at[tp, rows_of(flipped(ep, near, n)), lanes],
            sent_sem.at[5],
            recv_sem.at[near // 2 + m],
            (there, tp),
        )

    relay_order = list(range(CHUNK, near)) + list(range(1, CHUNK))

    def relay():
        raw_copies[0].wait_recv()
        first_slot = (ep // near) * (near * capacity)
        half_ids = lax.broadcasted_iota(jnp.int32, (near * capacity, tokens), 0) + first_slot
        half_pick = jnp.where(
            (half_ids == raw_info[0:1, :]) | (half_ids == raw_info[1:2, :]), 1.0, 0.0
        ).astype(jnp.bfloat16)
        for index, lanes in enumerate(relay_lanes):
            raw_copies[1 + index].wait_recv()
            relayed[:, lanes] = jnp.dot(
                half_pick, raw_rows[:, lanes], preferred_element_type=jnp.float32
            ).astype(jnp.bfloat16)
            for m in relay_order:
                relay_copy(m, lanes).start()
            arrived[tp, rows_of(flipped(ep, near, n)), lanes] = relayed[rows_of(ep % near), lanes]

    def sends_outer():
        for copy in raw_copies:
            copy.start()

    def sends_inner():
        for k in range(near, n):
            dispatch(k).start()

    def sent_outer():
        raw_copies[0].wait_send()
        all_sent(normed_v.at[tp], raw_sem.at[1])

    def sent_inner():
        all_sent(outgoing.at[0, pl.ds(0, near * capacity)], sent_sem.at[1])
        all_sent(relayed.at[pl.ds(0, (near - 1) * capacity)], sent_sem.at[5])

    for k in range(1, near):
        dispatch(k).start()
    pl.when(inner == 0)(sends_outer)
    pl.when(inner == 1)(sends_inner)
    arrived[:, own_rows] = outgoing[:, own_rows]

    def contract(left, right):
        return lax.dot_general(
            left, right, (((1,), (1,)), ((), ())), preferred_element_type=jnp.float32
        )

    def logits_of(router):
        return contract(router[:, :half], normed_v[0]) + contract(router[:, half:], normed_v[1])

    group_logits = logits_of(group_rt_ref)
    inner_logits = logits_of(inner_rt_ref)
    group_ids = lax.broadcasted_iota(jnp.int32, group_logits.shape, 0)
    own_logit = jnp.sum(
        jnp.where(group_ids == group_pick, group_logits, 0.0), axis=0, keepdims=True
    )
    share = 1.0 / jnp.sum(jnp.exp(group_logits - own_logit), axis=0, keepdims=True)
    picked = [
        jnp.sum(jnp.where(hit, inner_logits, 0.0), axis=0, keepdims=True) for hit in hits
    ]
    first = jax.nn.sigmoid(picked[0] - picked[1])
    weights = [
        (share * value).astype(jnp.bfloat16).astype(jnp.float32) for value in (first, 1.0 - first)
    ]
    spread = jnp.where(chosen[0], weights[0], 0.0) + jnp.where(chosen[1], weights[1], 0.0)
    combine_w[...] = spread.T.astype(jnp.bfloat16)

    def mixer():
        halo_copy.wait()
        group_width = mix_ref.shape[1] // 4
        position = linear * rows + lax.broadcasted_iota(jnp.int32, (rows, 1), 0)
        is_first = linear == 0
        for index in range(4):
            window = 2 ** (index + 1)
            lanes = slice(index * group_width, (index + 1) * group_width)
            lead = jnp.where(is_first, 0.0, halo[:, lanes].astype(jnp.float32))
            body = mix_ref[:, lanes].astype(jnp.float32)
            sums = jnp.concatenate([lead, body], axis=0)
            shift = 1
            while shift < window:
                sums = sums + pltpu.roll(sums, shift, 0)
                shift *= 2
            inverse = 1.0 / jnp.minimum(position + 1, window).astype(jnp.float32)
            pooled_v[:, lanes] = (sums[LEAD:] * inverse - body).astype(jnp.bfloat16)
        group_dim = pool_w_ref.shape[1]
        for g in range(pool_w_ref.shape[0]):
            lanes = slice(g * group_dim, (g + 1) * group_dim)
            product = jnp.dot(pooled_v[:, lanes], pool_w_ref[g], preferred_element_type=jnp.float32)
            grouped_v[:, lanes] = (product * pool_s_ref[:, lanes]).astype(jnp.bfloat16)
        loads[2].wait()
        tile = 512

        @pl.loop(0, mix_out_ref.shape[1] // tile)
        def _(step):
            lanes = pl.ds(pl.multiple_of(step * tile, tile), tile)
            mix_out_ref[:, lanes] = jnp.dot(
                grouped_v[...], out_w[:, lanes], preferred_element_type=jnp.float32
            ).astype(jnp.bfloat16)

    groups = [list(range(first, first + CHUNK)) for first in range(0, n, CHUNK)]

    def expert(group):
        size = len(group)
        start = partner(group[0])[1] // size * (size * capacity)
        span = pl.ds(pl.multiple_of(start, size * capacity), size * capacity)
        sums = []
        for weight in (gate_w, up_w):
            sums.append(
                jnp.dot(arrived[0, span], weight[:half], preferred_element_type=jnp.float32)
                + jnp.dot(arrived[1, span], weight[half:], preferred_element_type=jnp.float32)
            )
        hidden = (sums[0] / (1.0 + jnp.exp(-sums[0])) * sums[1]).astype(jnp.bfloat16)

        def part(index):
            return jnp.dot(
                hidden, down_w[index], preferred_element_type=jnp.float32
            ).astype(jnp.bfloat16)

        part_send[span] = part(other)
        for k in group:
            partial_copy(k).start()
        part_own[span] = part(tp)

    def finish(ks):
        for k in ks:
            block = rows_of(partner(k)[1])
            partial_copy(k).wait_recv()
            result[block] = (
                part_own[block].astype(jnp.float32) + part_recv[block].astype(jnp.float32)
            ).astype(jnp.bfloat16)
            if k:
                give_back(k).start()
            else:
                returned[block] = result[block]

    def pass_on(k):
        if k == near + CHUNK:
            pl.when(inner == 0)(dispatch(k).wait_recv)
        else:
            dispatch(k).wait_recv()
        swap(k).start()

    def straight(pair):
        if pair[0] == 0:
            dispatch(1).wait_recv()
        else:
            landed(arrived.at[:, pair_rows(pair[0])], recv_sem.at[pair[0] // 2])
        expert(pair)

    def swapped(pair):
        landed(arrived.at[other, pair_rows(pair[0])], swap_recv.at[(pair[0] - near) // 2])
        expert(pair)

    early, late, beside, beyond, far, farther, last, latest = [
        [first, first + 1] for first in range(0, n, 2)
    ]

    def late_plane():
        for k in late:
            dispatch(k).wait_recv()
            expert([k])

    def beyond_plane():
        straight(beyond)

    def beyond_back():
        finish(beyond)

    def late_back():
        finish(late)

    for index in (0, 1, 3, 4):
        loads[index].wait()
    straight(early)
    mixer()
    pl.when(inner == 0)(late_plane)
    for k in far + farther:
        pass_on(k)
    finish(early)
    pl.when(inner == 0)(late_back)
    swapped(far)
    swapped(farther)
    straight(beside)
    pl.when(inner == 1)(beyond_plane)
    finish(far)
    pl.when(inner == 1)(relay)
    finish(farther)
    for k in last + latest:
        pass_on(k)
    finish(beside)
    pl.when(inner == 1)(beyond_back)
    swapped(last)
    swapped(latest)
    pl.when(inner == 0)(beyond_plane)
    finish(last)
    pl.when(inner == 1)(late_plane)
    finish(latest)
    pl.when(inner == 0)(beyond_back)
    pl.when(inner == 1)(late_back)
    landed(returned.at[pl.ds(0, (n - 1) * capacity)], ret_recv.at[0])
    moe_out_ref[...] = jnp.dot(
        combine_w[...], returned[...], preferred_element_type=jnp.float32
    ).astype(jnp.bfloat16)
    pl.when(inner == 0)(sent_outer)
    pl.when(inner == 1)(sent_inner)
    all_sent(outgoing.at[:, pl.ds(0, (near - 1) * capacity)], sent_sem.at[0])
    all_sent(arrived.at[0, pl.ds(0, near * capacity)], sent_sem.at[2])
    all_sent(part_send, sent_sem.at[3])
    all_sent(result.at[pl.ds(0, (n - 1) * capacity)], sent_sem.at[4])


def fused(
    mix_input,
    pool_weight,
    pool_scale,
    out_weight,
    moe_input,
    moe_gain,
    group_router,
    inner_router,
    group_pick,
    inner_pick,
    gate_weight,
    up_weight,
    down_weight,
):
    n = lax.axis_size("ep")
    tokens, width = moe_input.shape
    rows, channels = mix_input.shape
    expert_count = inner_router.shape[1]
    capacity = 2 * inner_pick.shape[1] * tokens // expert_count
    half = width // 2
    slots = n * capacity
    hidden = gate_weight.shape[2]
    bf16 = jnp.bfloat16
    vmem = pl.BlockSpec(memory_space=pltpu.VMEM)
    hbm = pl.BlockSpec(memory_space=pl.ANY)
    dma = pltpu.SemaphoreType.DMA
    in_vmem = pl.pallas_call(
        functools.partial(
            fused_kernel, n, capacity, expert_count // group_router.shape[1]
        ),
        out_shape=(
            pltpu.VMEM((rows, out_weight.shape[1]), bf16),
            pltpu.VMEM((tokens, half), bf16),
        ),
        in_specs=[vmem, vmem, vmem, hbm] + [vmem] * 6 + [hbm] * 3,
        out_specs=(vmem, vmem),
        scratch_shapes=[
            pltpu.VMEM(out_weight.shape, bf16),
            pltpu.VMEM((width, hidden), bf16),
            pltpu.VMEM((width, hidden), bf16),
            pltpu.VMEM((2, hidden, half), bf16),
            pltpu.VMEM((LEAD, channels), bf16),
            pltpu.VMEM((rows, channels), bf16),
            pltpu.VMEM((rows, channels), bf16),
            pltpu.VMEM((2, tokens, half), bf16),
            pltpu.VMEM((2, slots, half), bf16),
            pltpu.VMEM((2, slots, half), bf16),
            pltpu.VMEM((slots, half), bf16),
            pltpu.VMEM((slots, half), bf16),
            pltpu.VMEM((slots, half), bf16),
            pltpu.VMEM((slots, half), bf16),
            pltpu.VMEM((slots, half), bf16),
            pltpu.VMEM((tokens, slots), bf16),
            pltpu.VMEM((2, tokens), jnp.int32),
            pltpu.VMEM((2, tokens), jnp.int32),
            pltpu.VMEM((tokens, half), bf16),
            pltpu.VMEM((slots // 2, half), bf16),
            dma((5,)),
            dma((2,)),
            dma((6,)),
            dma((n // 2 + n // 4 + 1,)),
            dma((n // 4,)),
            dma((n,)),
            dma((1,)),
            dma((5,)),
        ],
        compiler_params=pltpu.CompilerParams(
            collective_id=0, has_side_effects=True, vmem_limit_bytes=60 * 1024 * 1024
        ),
    )(
        mix_input,
        pool_weight,
        pool_scale[None, :],
        out_weight,
        moe_input,
        moe_gain[None, :],
        group_router.T,
        inner_router.T,
        group_pick[None, :],
        inner_pick.T,
        gate_weight,
        up_weight,
        down_weight,
    )
    return pl.pallas_call(
        write_out,
        out_shape=tuple(jax.ShapeDtypeStruct(value.shape, value.dtype) for value in in_vmem),
        in_specs=[hbm, hbm],
        out_specs=(hbm, hbm),
        scratch_shapes=[dma((2,))],
    )(*[pltpu.with_memory_space_constraint(value, pltpu.VMEM) for value in in_vmem])


def write_out(mix_vmem, moe_vmem, mix_hbm, moe_hbm, sem):
    copies = [
        pltpu.make_async_copy(mix_vmem, mix_hbm, sem.at[0]),
        pltpu.make_async_copy(moe_vmem, moe_hbm, sem.at[1]),
    ]
    for copy in copies:
        copy.start()
    for copy in copies:
        copy.wait()


def step(*arrays):
    mix_input, moe_input, inner_router, inner_pick = arrays[0], arrays[4], arrays[7], arrays[9]
    n, n_tp = lax.axis_size("ep"), lax.axis_size("tp")
    capacity = 2 * inner_pick.shape[1] * moe_input.shape[0] // inner_router.shape[1]
    fits = (
        n_tp == 2
        and inner_pick.shape[1] == 2
        and n == 4 * CHUNK
        and inner_router.shape[1] == n
        and capacity % 16 == 0
        and mix_input.shape[0] >= LEAD
    )
    return fused(*arrays) if fits else per_device(*arrays)


def solution(mesh):
    in_specs = (
        P(("ep", "tp"), None),
        P(),
        P(),
        P(),
        P("ep", None),
        P(),
        P(),
        P(),
        P("ep"),
        P("ep", None),
        P("ep", None, "tp"),
        P("ep", None, "tp"),
        P("ep", "tp", None),
    )
    out_specs = (P(("ep", "tp"), None), P("ep", "tp"))
    return jax.shard_map(
        step, mesh=mesh, in_specs=in_specs, out_specs=out_specs, check_vma=False
    )
```

```python
import functools

import jax
import jax.numpy as jnp
from jax import lax
from jax.experimental import pallas as pl
from jax.experimental.pallas import tpu as pltpu
from jax.sharding import PartitionSpec as P

MESH = pl.DeviceIdType.MESH
CHUNK = 4
LEAD = 16

WINDOW_MAX = 16


NORM_FLOOR = 0.25


def passed_along(value, axis, steps):
    count = lax.axis_size(axis)
    first, last = (max(0, -steps), min(count, count - steps))
    return lax.ppermute(value, axis, [(source, source + steps) for source in range(first, last)])


def trailing_means(extended, row_count, lead_rows, first_position):
    group_width = extended.shape[1] // 4
    position = first_position + jnp.arange(row_count, dtype=jnp.int32)
    pieces = []
    for scale_index in range(4):
        window = 2 ** (scale_index + 1)
        channel_block = extended[:, scale_index * group_width : (scale_index + 1) * group_width]
        window_sum = channel_block[lead_rows : lead_rows + row_count]
        for back_step in range(1, window):
            window_sum = (
                window_sum
                + channel_block[lead_rows - back_step : lead_rows - back_step + row_count]
            )
        divisor = jnp.minimum(position + 1, window).astype(jnp.float32)
        pieces.append(window_sum / divisor[:, None])
    return jnp.concatenate(pieces, axis=1)


def route_terms(group_logits, inner_logits, group_pick, inner_pick, per_group):
    group_ids = jnp.arange(group_logits.shape[1], dtype=jnp.int32)
    chosen = jnp.sum(
        jnp.where(group_pick[:, None] == group_ids[None, :], group_logits, 0.0), axis=1
    )
    group_share = 1.0 / jnp.sum(jnp.exp(group_logits - chosen[:, None]), axis=1)
    target = group_pick[:, None] * per_group + inner_pick
    expert_ids = jnp.arange(inner_logits.shape[1], dtype=jnp.int32)
    picked = jnp.sum(
        jnp.where(target[:, :, None] == expert_ids[None, None, :], inner_logits[:, None, :], 0.0),
        axis=2,
    )
    first_share = jax.nn.sigmoid(picked[:, 0] - picked[:, 1])
    route_weight = group_share[:, None] * jnp.stack([first_share, 1.0 - first_share], axis=1)
    return (target, route_weight)


def slot_terms(target, expert_count, capacity):
    expert_ids = jnp.arange(expert_count, dtype=jnp.int32)
    expert_hits = (target[:, :, None] == expert_ids[None, None, :]).astype(jnp.int32)
    per_token = jnp.sum(expert_hits, axis=1)
    earlier = jnp.cumsum(per_token, axis=0) - per_token
    route_rank = jnp.sum(expert_hits * earlier[:, None, :], axis=2)
    is_kept = route_rank < capacity
    slot_index = target * capacity + jnp.minimum(route_rank, capacity - 1)
    return (slot_index, is_kept)


def slot_sources(slot_index, is_kept, slot_count):
    token_ids = jnp.broadcast_to(
        jnp.arange(slot_index.shape[0], dtype=jnp.int32)[:, None], slot_index.shape
    )
    placed = jnp.where(is_kept, slot_index, slot_count).reshape(-1)
    source = jnp.zeros((slot_count,), jnp.int32).at[placed].set(token_ids.reshape(-1), mode="drop")
    slot_used = jnp.zeros((slot_count,), jnp.bool_).at[placed].set(True, mode="drop")
    return (source, slot_used)


def per_device(
    mix_input,
    pool_weight,
    pool_scale,
    out_weight,
    moe_input,
    moe_gain,
    group_router,
    inner_router,
    group_pick,
    inner_pick,
    gate_weight,
    up_weight,
    down_weight,
):
    row_count = mix_input.shape[0]
    reach_back = WINDOW_MAX - 1
    before = passed_along(mix_input[row_count - reach_back :], ("ep", "tp"), 1)
    extended = jnp.concatenate([before, mix_input], axis=0).astype(jnp.float32)
    first_position = lax.axis_index(("ep", "tp")) * row_count
    trailing = (
        trailing_means(extended, row_count, reach_back, first_position) - extended[reach_back:]
    )
    pooled = trailing.astype(jnp.bfloat16)
    groups, group_dim = (pool_weight.shape[0], pool_weight.shape[1])
    grouped = jnp.einsum(
        "tgc,gcd->tgd",
        pooled.reshape(row_count, groups, group_dim),
        pool_weight,
        preferred_element_type=jnp.float32,
    )
    grouped = (grouped.reshape(row_count, groups * group_dim) * pool_scale[None, :]).astype(
        jnp.bfloat16
    )
    mix_out = jnp.dot(grouped, out_weight, preferred_element_type=jnp.float32).astype(jnp.bfloat16)
    tokens, feature_width = moe_input.shape
    token_values = moe_input.astype(jnp.float32)
    norm_scale = lax.rsqrt(
        jnp.maximum(jnp.mean(token_values * token_values, axis=1, keepdims=True), NORM_FLOOR)
    )
    normed = (token_values * norm_scale * moe_gain[None, :]).astype(jnp.bfloat16)
    group_logits = jnp.dot(normed, group_router, preferred_element_type=jnp.float32)
    inner_logits = jnp.dot(normed, inner_router, preferred_element_type=jnp.float32)
    group_count = group_router.shape[1]
    expert_count = inner_router.shape[1]
    target, route_weight = route_terms(
        group_logits, inner_logits, group_pick, inner_pick, expert_count // group_count
    )
    capacity = 2 * inner_pick.shape[1] * tokens // expert_count
    slot_index, is_kept = slot_terms(target, expert_count, capacity)
    source, slot_used = slot_sources(slot_index, is_kept, expert_count * capacity)
    gate_local = gate_weight[0]
    up_local = up_weight[0]
    outgoing = jnp.where(slot_used[:, None], normed[source], jnp.zeros((), jnp.bfloat16))
    arrived = lax.all_to_all(outgoing, "ep", split_axis=0, concat_axis=0, tiled=True)
    gate_sum = jnp.dot(arrived, gate_local, preferred_element_type=jnp.float32)
    up_sum = jnp.dot(arrived, up_local, preferred_element_type=jnp.float32)
    hidden = (jax.nn.silu(gate_sum) * up_sum).astype(jnp.bfloat16)
    down_local = down_weight[0]
    expert_result = lax.psum_scatter(
        lax.dot_general(
            down_local, hidden, (((0,), (1,)), ((), ())), preferred_element_type=jnp.float32
        ).astype(jnp.bfloat16),
        "tp",
        scatter_dimension=0,
        tiled=True,
    )
    returned = lax.all_to_all(expert_result, "ep", split_axis=1, concat_axis=1, tiled=True)
    route_scale = jnp.where(is_kept, route_weight, 0.0).astype(jnp.bfloat16)
    route_scale = lax.optimization_barrier(route_scale).astype(jnp.float32)
    picked = jnp.take(returned, slot_index, axis=1).astype(jnp.float32)
    combined = jnp.sum(picked * route_scale[None, :, :], axis=2)
    moe_out = combined.T.astype(jnp.bfloat16)
    return (mix_out, moe_out)


def flipped(index, mask, count):
    total = 0
    bit = 1
    while bit < count:
        own = (index // bit) % 2
        total = total + bit * ((1 - own) if mask & bit else own)
        bit *= 2
    return total


def fused_kernel(
    n,
    capacity,
    per_group,
    mix_hbm,
    pool_w_hbm,
    pool_s_hbm,
    out_w_hbm,
    moe_hbm,
    gain_hbm,
    group_rt_hbm,
    inner_rt_hbm,
    gp_hbm,
    ip_hbm,
    gate_hbm,
    up_hbm,
    down_hbm,
    mix_out_ref,
    moe_out_ref,
    moe_ref,
    gain_ref,
    gp_ref,
    ip_ref,
    mix_ref,
    group_rt_ref,
    inner_rt_ref,
    pool_w_ref,
    pool_s_ref,
    input_sem,
    out_w,
    gate_w,
    up_w,
    down_w,
    halo,
    pooled_v,
    grouped_v,
    normed_v,
    outgoing,
    arrived,
    part_own,
    part_send,
    part_recv,
    result,
    returned,
    combine_w,
    slot_info,
    raw_info,
    raw_rows,
    relayed,
    load_sem,
    halo_sem,
    sent_sem,
    recv_sem,
    swap_recv,
    part_recv_sem,
    ret_recv,
    raw_sem,
):
    ep, tp = lax.axis_index("ep"), lax.axis_index("tp")
    other = 1 - tp
    total_devices = 2 * n
    linear = ep * 2 + tp
    following = lax.rem(linear + 1, total_devices)
    preceding = lax.rem(linear + total_devices - 1, total_devices)
    tokens, width = moe_ref.shape
    half = width // 2
    rows = mix_ref.shape[0]
    slots = n * capacity
    near = n // 2
    low, high = (ep // CHUNK) % 2, (ep // near) % 2
    inner = low + high - 2 * low * high

    barrier = pltpu.get_barrier_semaphore()
    greeted = [(flipped(ep, j, n), tp) for j in range(1, n)]
    greeted += [(ep, other), (following // 2, following % 2), (preceding // 2, preceding % 2)]
    for device in greeted:
        pl.semaphore_signal(barrier, inc=1, device_id=device, device_id_type=MESH)

    inputs = [
        pltpu.make_async_copy(source, target, input_sem.at[index])
        for index, (source, target) in enumerate(
            [
                (moe_hbm, moe_ref),
                (gain_hbm, gain_ref),
                (gp_hbm, gp_ref),
                (ip_hbm, ip_ref),
                (mix_hbm, mix_ref),
                (group_rt_hbm, group_rt_ref),
                (inner_rt_hbm, inner_rt_ref),
                (pool_w_hbm, pool_w_ref),
                (pool_s_hbm, pool_s_ref),
            ]
        )
    ]
    for load in inputs:
        load.start()
    loads = [
        pltpu.make_async_copy(gate_hbm.at[0], gate_w, load_sem.at[0]),
        pltpu.make_async_copy(up_hbm.at[0], up_w, load_sem.at[1]),
        pltpu.make_async_copy(out_w_hbm, out_w, load_sem.at[2]),
        pltpu.make_async_copy(down_hbm.at[0, :, pl.ds(0, half)], down_w.at[0], load_sem.at[3]),
        pltpu.make_async_copy(down_hbm.at[0, :, pl.ds(half, half)], down_w.at[1], load_sem.at[4]),
    ]
    for index in (0, 1, 3, 4, 2):
        loads[index].start()

    for load in inputs[:4]:
        load.wait()
    values = moe_ref[...].astype(jnp.float32)
    scale = lax.rsqrt(
        jnp.maximum(jnp.sum(values * values, axis=1, keepdims=True) * (1.0 / width), NORM_FLOOR)
    )
    normed = (values * scale * gain_ref[...]).astype(jnp.bfloat16)
    for part in range(2):
        normed_v[part] = normed[:, part * half : (part + 1) * half]

    group_pick = gp_ref[...]
    expert_count = inner_rt_ref.shape[0]
    targets = [group_pick * per_group + ip_ref[k : k + 1, :] for k in range(2)]
    expert_ids = lax.broadcasted_iota(jnp.int32, (expert_count, tokens), 0)
    hits = [expert_ids == target for target in targets]
    both = (hits[0].astype(jnp.float32) + hits[1].astype(jnp.float32)).astype(jnp.bfloat16)
    earlier_mask = (
        lax.broadcasted_iota(jnp.int32, (tokens, tokens), 0)
        < lax.broadcasted_iota(jnp.int32, (tokens, tokens), 1)
    ).astype(jnp.float32).astype(jnp.bfloat16)
    earlier = jnp.dot(both, earlier_mask, preferred_element_type=jnp.float32)
    slot_of = []
    for k in range(2):
        rank = jnp.sum(jnp.where(hits[k], earlier, 0.0), axis=0, keepdims=True).astype(jnp.int32)
        slot_of.append(jnp.where(rank < capacity, targets[k] * capacity + rank, -1))
    slot_ids = lax.broadcasted_iota(jnp.int32, (slots, tokens), 0)
    chosen = [slot_ids == slot for slot in slot_of]
    pick = jnp.where(chosen[0] | chosen[1], 1.0, 0.0).astype(jnp.bfloat16)
    for part in range(2):
        outgoing[part] = jnp.dot(
            pick, normed_v[part], preferred_element_type=jnp.float32
        ).astype(jnp.bfloat16)
    for k in range(2):
        slot_info[k : k + 1, :] = slot_of[k]

    pl.semaphore_wait(barrier, len(greeted))

    own_rows = pl.ds(pl.multiple_of(ep * capacity, capacity), capacity)
    halo_copy = pltpu.make_async_remote_copy(
        src_ref=mix_ref.at[pl.ds(rows - LEAD, LEAD)],
        dst_ref=halo,
        send_sem=halo_sem.at[0],
        recv_sem=halo_sem.at[1],
        device_id=(following // 2, following % 2),
        device_id_type=MESH,
    )
    inputs[4].wait()
    halo_copy.start()

    relay_lanes = [slice(0, half)]

    def rows_of(index):
        return pl.ds(pl.multiple_of(index * capacity, capacity), capacity)

    def partner(k):
        there = flipped(ep, k, n)
        if k < near:
            return k, there
        shift = CHUNK if k < near + CHUNK else -CHUNK
        return k + inner * shift, there + inner * (CHUNK - 2 * CHUNK * ((there // CHUNK) % 2))

    def pair_rows(k):
        start = partner(k)[1] // 2 * (2 * capacity)
        return pl.ds(pl.multiple_of(start, 2 * capacity), 2 * capacity)

    def remote(src, dst, sent, received, device):
        return pltpu.make_async_remote_copy(
            src_ref=src,
            dst_ref=dst,
            send_sem=sent,
            recv_sem=received,
            device_id=device,
            device_id_type=MESH,
        )

    def landed(ref, semaphore):
        remote(ref, ref, sent_sem.at[0], semaphore, (ep, other)).wait_recv()

    def all_sent(ref, semaphore):
        remote(ref, ref, semaphore, ret_recv.at[0], (ep, other)).wait_send()

    def dispatch(k):
        j, there = partner(k)
        if k < near:
            src, dst = outgoing.at[:, rows_of(there)], arrived.at[:, own_rows]
            sent, received = sent_sem.at[0], recv_sem.at[near // 2 + near if k == 2 else k // 2]
        else:
            src, dst = outgoing.at[tp, rows_of(there)], arrived.at[tp, own_rows]
            sent, received = sent_sem.at[1], recv_sem.at[near // 2 + j - near]
        return remote(src, dst, sent, received, (there, tp))

    def swap(k):
        block = arrived.at[tp, rows_of(partner(k)[1])]
        received = swap_recv.at[(k - near) // 2]
        return remote(block, block, sent_sem.at[2], received, (ep, other))

    def partial_copy(k):
        block = rows_of(partner(k)[1])
        received = part_recv_sem.at[k]
        return remote(
            part_send.at[block], part_recv.at[block], sent_sem.at[3], received, (ep, other)
        )

    def give_back(k):
        there = partner(k)[1]
        return remote(
            result.at[rows_of(there)],
            returned.at[own_rows],
            sent_sem.at[4],
            ret_recv.at[0],
            (there, tp),
        )

    raw_copies = [
        remote(src, dst, raw_sem.at[min(index, 1)], raw_sem.at[2 + index], (flipped(ep, near, n), tp))
        for index, (src, dst) in enumerate(
            [(slot_info, raw_info)]
            + [(normed_v.at[tp, :, lanes], raw_rows.at[:, lanes]) for lanes in relay_lanes]
        )
    ]

    def relay_copy(m, lanes):
        there = flipped(ep, m, n)
        return remote(
            relayed.at[rows_of(there % near), lanes],
            arrived.at[tp, rows_of(flipped(ep, near, n)), lanes],
            sent_sem.at[5],
            recv_sem.at[near // 2 + m],
            (there, tp),
        )

    relay_order = list(range(CHUNK, near)) + list(range(1, CHUNK))

    def relay():
        raw_copies[0].wait_recv()
        first_slot = (ep // near) * (near * capacity)
        half_ids = lax.broadcasted_iota(jnp.int32, (near * capacity, tokens), 0) + first_slot
        half_pick = jnp.where(
            (half_ids == raw_info[0:1, :]) | (half_ids == raw_info[1:2, :]), 1.0, 0.0
        ).astype(jnp.bfloat16)
        for index, lanes in enumerate(relay_lanes):
            raw_copies[1 + index].wait_recv()
            relayed[:, lanes] = jnp.dot(
                half_pick, raw_rows[:, lanes], preferred_element_type=jnp.float32
            ).astype(jnp.bfloat16)
            for m in relay_order:
                relay_copy(m, lanes).start()
            arrived[tp, rows_of(flipped(ep, near, n)), lanes] = relayed[rows_of(ep % near), lanes]

    def sends_outer():
        for copy in raw_copies:
            copy.start()

    def sends_inner():
        for k in range(near, n):
            dispatch(k).start()

    def sent_outer():
        raw_copies[0].wait_send()
        all_sent(normed_v.at[tp], raw_sem.at[1])

    def sent_inner():
        all_sent(outgoing.at[0, pl.ds(0, near * capacity)], sent_sem.at[1])
        all_sent(relayed.at[pl.ds(0, (near - 1) * capacity)], sent_sem.at[5])

    for k in range(1, near):
        dispatch(k).start()
    pl.when(inner == 0)(sends_outer)
    pl.when(inner == 1)(sends_inner)
    arrived[:, own_rows] = outgoing[:, own_rows]

    def contract(left, right):
        return lax.dot_general(
            left, right, (((1,), (1,)), ((), ())), preferred_element_type=jnp.float32
        )

    def logits_of(router):
        return contract(router[:, :half], normed_v[0]) + contract(router[:, half:], normed_v[1])

    for load in inputs[5:]:
        load.wait()
    group_logits = logits_of(group_rt_ref)
    inner_logits = logits_of(inner_rt_ref)
    group_ids = lax.broadcasted_iota(jnp.int32, group_logits.shape, 0)
    own_logit = jnp.sum(
        jnp.where(group_ids == group_pick, group_logits, 0.0), axis=0, keepdims=True
    )
    share = 1.0 / jnp.sum(jnp.exp(group_logits - own_logit), axis=0, keepdims=True)
    picked = [
        jnp.sum(jnp.where(hit, inner_logits, 0.0), axis=0, keepdims=True) for hit in hits
    ]
    first = jax.nn.sigmoid(picked[0] - picked[1])
    weights = [
        (share * value).astype(jnp.bfloat16).astype(jnp.float32) for value in (first, 1.0 - first)
    ]
    spread = jnp.where(chosen[0], weights[0], 0.0) + jnp.where(chosen[1], weights[1], 0.0)
    combine_w[...] = spread.T.astype(jnp.bfloat16)

    def mixer():
        halo_copy.wait()
        group_width = mix_ref.shape[1] // 4
        position = linear * rows + lax.broadcasted_iota(jnp.int32, (rows, 1), 0)
        is_first = linear == 0
        for index in range(4):
            window = 2 ** (index + 1)
            lanes = slice(index * group_width, (index + 1) * group_width)
            lead = jnp.where(is_first, 0.0, halo[:, lanes].astype(jnp.float32))
            body = mix_ref[:, lanes].astype(jnp.float32)
            sums = jnp.concatenate([lead, body], axis=0)
            shift = 1
            while shift < window:
                sums = sums + pltpu.roll(sums, shift, 0)
                shift *= 2
            inverse = 1.0 / jnp.minimum(position + 1, window).astype(jnp.float32)
            pooled_v[:, lanes] = (sums[LEAD:] * inverse - body).astype(jnp.bfloat16)
        group_dim = pool_w_ref.shape[1]
        for g in range(pool_w_ref.shape[0]):
            lanes = slice(g * group_dim, (g + 1) * group_dim)
            product = jnp.dot(pooled_v[:, lanes], pool_w_ref[g], preferred_element_type=jnp.float32)
            grouped_v[:, lanes] = (product * pool_s_ref[:, lanes]).astype(jnp.bfloat16)
        loads[2].wait()
        tile = 512

        @pl.loop(0, mix_out_ref.shape[1] // tile)
        def _(step):
            lanes = pl.ds(pl.multiple_of(step * tile, tile), tile)
            mix_out_ref[:, lanes] = jnp.dot(
                grouped_v[...], out_w[:, lanes], preferred_element_type=jnp.float32
            ).astype(jnp.bfloat16)

    groups = [list(range(first, first + CHUNK)) for first in range(0, n, CHUNK)]

    def expert(group):
        size = len(group)
        start = partner(group[0])[1] // size * (size * capacity)
        span = pl.ds(pl.multiple_of(start, size * capacity), size * capacity)
        sums = []
        for weight in (gate_w, up_w):
            sums.append(
                jnp.dot(arrived[0, span], weight[:half], preferred_element_type=jnp.float32)
                + jnp.dot(arrived[1, span], weight[half:], preferred_element_type=jnp.float32)
            )
        hidden = (sums[0] / (1.0 + jnp.exp(-sums[0])) * sums[1]).astype(jnp.bfloat16)

        def part(index):
            return jnp.dot(
                hidden, down_w[index], preferred_element_type=jnp.float32
            ).astype(jnp.bfloat16)

        part_send[span] = part(other)
        for k in group:
            partial_copy(k).start()
        part_own[span] = part(tp)

    def finish(ks):
        for k in ks:
            block = rows_of(partner(k)[1])
            partial_copy(k).wait_recv()
            result[block] = (
                part_own[block].astype(jnp.float32) + part_recv[block].astype(jnp.float32)
            ).astype(jnp.bfloat16)
            if k:
                give_back(k).start()
            else:
                returned[block] = result[block]

    def pass_on(k):
        if k == near + CHUNK:
            pl.when(inner == 0)(dispatch(k).wait_recv)
        else:
            dispatch(k).wait_recv()
        swap(k).start()

    def straight(pair):
        if pair[0] == 0:
            dispatch(1).wait_recv()
        else:
            landed(arrived.at[:, pair_rows(pair[0])], recv_sem.at[pair[0] // 2])
        expert(pair)

    def swapped(pair):
        landed(arrived.at[other, pair_rows(pair[0])], swap_recv.at[(pair[0] - near) // 2])
        expert(pair)

    early, late, beside, beyond, far, farther, last, latest = [
        [first, first + 1] for first in range(0, n, 2)
    ]

    def late_plane():
        for k in late:
            dispatch(k).wait_recv()
            expert([k])

    def beyond_plane():
        straight(beyond)

    def beyond_back():
        finish(beyond)

    def late_back():
        finish(late)

    for index in (0, 1, 3, 4):
        loads[index].wait()
    straight(early)
    mixer()
    pl.when(inner == 0)(late_plane)
    for k in far + farther:
        pass_on(k)
    finish(early)
    pl.when(inner == 0)(late_back)
    swapped(far)
    swapped(farther)
    straight(beside)
    pl.when(inner == 1)(beyond_plane)
    finish(far)
    pl.when(inner == 1)(relay)
    finish(farther)
    for k in last + latest:
        pass_on(k)
    finish(beside)
    pl.when(inner == 1)(beyond_back)
    swapped(last)
    swapped(latest)
    pl.when(inner == 0)(beyond_plane)
    finish(last)
    pl.when(inner == 1)(late_plane)
    finish(latest)
    pl.when(inner == 0)(beyond_back)
    pl.when(inner == 1)(late_back)
    landed(returned.at[pl.ds(0, (n - 1) * capacity)], ret_recv.at[0])
    moe_out_ref[...] = jnp.dot(
        combine_w[...], returned[...], preferred_element_type=jnp.float32
    ).astype(jnp.bfloat16)
    pl.when(inner == 0)(sent_outer)
    pl.when(inner == 1)(sent_inner)
    all_sent(outgoing.at[:, pl.ds(0, (near - 1) * capacity)], sent_sem.at[0])
    all_sent(arrived.at[0, pl.ds(0, near * capacity)], sent_sem.at[2])
    all_sent(part_send, sent_sem.at[3])
    all_sent(result.at[pl.ds(0, (n - 1) * capacity)], sent_sem.at[4])


def fused(
    mix_input,
    pool_weight,
    pool_scale,
    out_weight,
    moe_input,
    moe_gain,
    group_router,
    inner_router,
    group_pick,
    inner_pick,
    gate_weight,
    up_weight,
    down_weight,
):
    n = lax.axis_size("ep")
    tokens, width = moe_input.shape
    rows, channels = mix_input.shape
    expert_count = inner_router.shape[1]
    capacity = 2 * inner_pick.shape[1] * tokens // expert_count
    half = width // 2
    slots = n * capacity
    hidden = gate_weight.shape[2]
    bf16 = jnp.bfloat16
    vmem = pl.BlockSpec(memory_space=pltpu.VMEM)
    hbm = pl.BlockSpec(memory_space=pl.ANY)
    dma = pltpu.SemaphoreType.DMA
    in_vmem = pl.pallas_call(
        functools.partial(
            fused_kernel, n, capacity, expert_count // group_router.shape[1]
        ),
        out_shape=(
            pltpu.VMEM((rows, out_weight.shape[1]), bf16),
            pltpu.VMEM((tokens, half), bf16),
        ),
        in_specs=[hbm] * 13,
        out_specs=(vmem, vmem),
        scratch_shapes=[
            pltpu.VMEM((tokens, width), bf16),
            pltpu.VMEM((1, width), moe_gain.dtype),
            pltpu.VMEM((1, tokens), group_pick.dtype),
            pltpu.VMEM((inner_pick.shape[1], tokens), inner_pick.dtype),
            pltpu.VMEM((rows, channels), bf16),
            pltpu.VMEM(group_router.T.shape, bf16),
            pltpu.VMEM(inner_router.T.shape, bf16),
            pltpu.VMEM(pool_weight.shape, bf16),
            pltpu.VMEM((1, channels), pool_scale.dtype),
            dma((9,)),
            pltpu.VMEM(out_weight.shape, bf16),
            pltpu.VMEM((width, hidden), bf16),
            pltpu.VMEM((width, hidden), bf16),
            pltpu.VMEM((2, hidden, half), bf16),
            pltpu.VMEM((LEAD, channels), bf16),
            pltpu.VMEM((rows, channels), bf16),
            pltpu.VMEM((rows, channels), bf16),
            pltpu.VMEM((2, tokens, half), bf16),
            pltpu.VMEM((2, slots, half), bf16),
            pltpu.VMEM((2, slots, half), bf16),
            pltpu.VMEM((slots, half), bf16),
            pltpu.VMEM((slots, half), bf16),
            pltpu.VMEM((slots, half), bf16),
            pltpu.VMEM((slots, half), bf16),
            pltpu.VMEM((slots, half), bf16),
            pltpu.VMEM((tokens, slots), bf16),
            pltpu.VMEM((2, tokens), jnp.int32),
            pltpu.VMEM((2, tokens), jnp.int32),
            pltpu.VMEM((tokens, half), bf16),
            pltpu.VMEM((slots // 2, half), bf16),
            dma((5,)),
            dma((2,)),
            dma((6,)),
            dma((n // 2 + n // 4 + 1,)),
            dma((n // 4,)),
            dma((n,)),
            dma((1,)),
            dma((5,)),
        ],
        compiler_params=pltpu.CompilerParams(
            collective_id=0, has_side_effects=True, vmem_limit_bytes=60 * 1024 * 1024
        ),
    )(
        mix_input,
        pool_weight,
        pool_scale[None, :],
        out_weight,
        moe_input,
        moe_gain[None, :],
        group_router.T,
        inner_router.T,
        group_pick[None, :],
        inner_pick.T,
        gate_weight,
        up_weight,
        down_weight,
    )
    return pl.pallas_call(
        write_out,
        out_shape=tuple(jax.ShapeDtypeStruct(value.shape, value.dtype) for value in in_vmem),
        in_specs=[hbm, hbm],
        out_specs=(hbm, hbm),
        scratch_shapes=[dma((2,))],
    )(*[pltpu.with_memory_space_constraint(value, pltpu.VMEM) for value in in_vmem])


def write_out(mix_vmem, moe_vmem, mix_hbm, moe_hbm, sem):
    copies = [
        pltpu.make_async_copy(mix_vmem, mix_hbm, sem.at[0]),
        pltpu.make_async_copy(moe_vmem, moe_hbm, sem.at[1]),
    ]
    for copy in copies:
        copy.start()
    for copy in copies:
        copy.wait()


def step(*arrays):
    mix_input, moe_input, inner_router, inner_pick = arrays[0], arrays[4], arrays[7], arrays[9]
    n, n_tp = lax.axis_size("ep"), lax.axis_size("tp")
    capacity = 2 * inner_pick.shape[1] * moe_input.shape[0] // inner_router.shape[1]
    fits = (
        n_tp == 2
        and inner_pick.shape[1] == 2
        and n == 4 * CHUNK
        and inner_router.shape[1] == n
        and capacity % 16 == 0
        and mix_input.shape[0] >= LEAD
    )
    return fused(*arrays) if fits else per_device(*arrays)


def solution(mesh):
    in_specs = (
        P(("ep", "tp"), None),
        P(),
        P(),
        P(),
        P("ep", None),
        P(),
        P(),
        P(),
        P("ep"),
        P("ep", None),
        P("ep", None, "tp"),
        P("ep", None, "tp"),
        P("ep", "tp", None),
    )
    out_specs = (P(("ep", "tp"), None), P("ep", "tp"))
    return jax.shard_map(
        step, mesh=mesh, in_specs=in_specs, out_specs=out_specs, check_vma=False
    )
```
